32 devices in a mesh: sp: 8 (over z, y), tp: 4 (over x, core).
Axes of the slice: x: 2, y: 2, z: 4, core: 2. Of those that a mesh axis runs over, the one named last changes fastest.
Arguments:
- stream_in: bfloat16 [2048, 2048], P(('sp', 'tp')), may hold values from -6 to 6
- queries_one: bfloat16 [2048, 1024], P('sp', 'tp'), may hold values from -120 to 120
- queries_two: bfloat16 [2048, 1024], P('sp', 'tp'), may hold values from -120 to 120
- keys_one: bfloat16 [2048, 512], P('sp', 'tp'), may hold values from -7 to 7
- keys_two: bfloat16 [2048, 512], P('sp', 'tp'), may hold values from -7 to 7
- values: bfloat16 [2048, 1024], P('sp', 'tp'), may hold values from -6 to 6
- lambdas: float32 [8], P('tp'), may hold values from 0.3 to 0.8
- head_gain: float32 [256], replicated, may hold values from 0.1 to 1.9
- out_weight: bfloat16 [2048, 2048], P('tp'), may hold values from -0.125 to 0.125
- norm_gain: float32 [2048], replicated, may hold values from 0.1 to 1.9
- expert_ids: int32 [2048, 2], P(('sp', 'tp')), may hold values from 0 to 7, all different within a row; in each aligned block of 64 rows (0 to 63, 64 to 127, ...) at most 32 rows name the same one
- route_weight: float32 [2048, 2], P(('sp', 'tp')), may hold values from 0.1 to 1
- gate_weight: bfloat16 [8, 2048, 1024], P('sp', None, 'tp'), may hold values from -0.125 to 0.125
- up_weight: bfloat16 [8, 2048, 1024], P('sp', None, 'tp'), may hold values from -0.125 to 0.125
- down_weight: bfloat16 [8, 1024, 2048], P('sp', 'tp'), may hold values from -0.1875 to 0.1875
Outputs:
- mixed: bfloat16 [2048, 2048], P(('sp', 'tp'))
The draws below stay inside these ranges and needn't reach their ends.
Inputs may be any that keep to these rules, and one draw needn't show every extreme that they name: `expert_ids`: each row names 2 different experts. In each aligned block of 64 rows no expert is named more than 32 times, a bound that some block reaches.
All inputs are finite; a program needn't handle non-finite values.
Results may differ from the reference program's by a relative error of at most 0.013.
Values may be sent and summed in bfloat16 or wider, within the bound.
A program may use at most 128 MiB of HBM per device.

```python
import math
import jax
import jax.numpy as jnp
import numpy as np
from jax import lax

D = 2048
HEADS = 8
KV_HEADS = 4
HEAD_DIM = 128
VAL_DIM = 256
EXPERT_FF = 1024
TOPK = 2
TOKENS = 2048
ROWS_DEV = 64
EXPERTS = 8
CAP = 32
N_SP = 8
N_TP = 4


def attention_draw(key):
    keys_first = jnp.clip(jax.random.normal(jax.random.fold_in(key, 11), (TOKENS, KV_HEADS * HEAD_DIM), jnp.float32) * 1.2, -7.0, 7.0)
    keys_second = jnp.clip(jax.random.normal(jax.random.fold_in(key, 12), (TOKENS, KV_HEADS * HEAD_DIM), jnp.float32) * 1.2, -7.0, 7.0)
    query_first = jnp.clip(jax.random.normal(jax.random.fold_in(key, 13), (TOKENS, HEADS * HEAD_DIM), jnp.float32) * 1.5, -9.0, 9.0)
    query_second = jnp.clip(jax.random.normal(jax.random.fold_in(key, 14), (TOKENS, HEADS * HEAD_DIM), jnp.float32) * 1.5, -9.0, 9.0)
    return (query_first, query_second, keys_first, keys_second)


def draw_queries_one(key, part):
    return attention_draw(key)[0].astype(jnp.bfloat16)


def draw_queries_two(key, part):
    return attention_draw(key)[1].astype(jnp.bfloat16)


def draw_keys_one(key, part):
    return attention_draw(key)[2].astype(jnp.bfloat16)


def draw_keys_two(key, part):
    return attention_draw(key)[3].astype(jnp.bfloat16)


def steps_of(key, dims, pieces, low, top_value):
    def one(position, blocks):
        heights = jax.random.uniform(jax.random.fold_in(jax.random.fold_in(key, 6), position), (blocks,), jnp.float32, low / len(pieces), top_value / len(pieces))
        return jnp.repeat(jnp.exp(heights), dims[position] // blocks).reshape((-1,) + (1,) * (len(dims) - position - 1))

    gain = one(*pieces[0])
    for cut in pieces[1:]:
        gain = gain * one(*cut)
    return gain


def deal_out(stream_key, own, number, rows, number_of, top, limit, lean):
    ranking = jax.random.permutation(stream_key, number_of)
    crowded, ordinary = shares(number_of, rows * top, limit, lean, True), shares(number_of, rows * top, limit, lean, False)
    places = jnp.arange(number_of)

    def named(lengths, turn):
        used = int((lengths > 0).sum())
        fixed = max(1, used // 4)
        shifted = fixed + (places - fixed + turn * (used - fixed)) % max(1, number_of - fixed)
        return jnp.zeros((number_of,), jnp.int32).at[ranking[jnp.where(places < fixed, places, shifted)]].set(jnp.asarray(lengths, jnp.int32))

    lengths = jnp.where(number % 4 == 0, named(crowded, number // 4), named(ordinary, number - number // 4 - 1))
    mixed = jax.random.permutation(jax.random.fold_in(own, 3), number_of)
    giver, receiver = mixed[0:number_of // 2 * 2:2], mixed[1:number_of // 2 * 2:2]
    room = jnp.minimum(lengths[giver] - 1, limit - lengths[receiver]) // 2
    room = jnp.where((giver == ranking[0]) | (receiver == ranking[0]) | (lengths[receiver] == 0), 0, jnp.maximum(room, 0))
    shifted = jax.random.randint(jax.random.fold_in(own, 4), (number_of // 2,), 0, 1 << 20) % (room + 1)
    lengths = lengths.at[giver].add(-shifted).at[receiver].add(shifted)
    labels = jnp.searchsorted(jnp.cumsum(lengths), jnp.arange(rows * top), side="right").astype(jnp.int32)
    listing = labels.reshape(top, rows).T
    listing = listing[jax.random.permutation(jax.random.fold_in(own, 1), rows)]
    turn = jax.random.randint(jax.random.fold_in(own, 2), (rows, 1), 0, top)
    return jnp.take_along_axis(listing, (jnp.arange(top)[None, :] + turn) % top, axis=1)


def shares(count, total, limit, slope, full):
    loads = [(1 << 20) // math.isqrt(grade ** slope) + 1 for grade in range(1, count + 1)]
    largest = limit if full else min(limit, max(-(-total // count), total * loads[0] // sum(loads)))
    least = 1 if total - largest >= count - 1 else 0
    given, rest = [largest] + [least] * (count - 1), total - largest - least * (count - 1)
    while rest > 0:
        free = [i for i in range(1, count) if given[i] < largest] or [i for i in range(1, count) if given[i] < limit]
        whole, left = sum([loads[i] for i in free]), rest
        for i in free:
            more = min(limit - given[i], max(1, left * loads[i] // whole), rest)
            given[i] = given[i] + more
            rest = rest - more
    return np.array(given)


def gaussian(stream_key, extent, width, bound, split=(), kind=jnp.bfloat16):
    entries = jax.random.normal(stream_key, extent, jnp.float32) * width
    if len(split) > 0:
        entries = steps_of(stream_key, extent, split, -0.22, 0.18) * entries
    return jnp.clip(entries, min=-bound, max=bound).astype(kind)


def setup_inputs(seed: int = 0) -> dict:
    seeds = jax.random.split(jax.random.key(seed), 16)
    stream_in = gaussian(seeds[0], (TOKENS, D), 1.0, 6.0, ((0, 32),))
    queries_one = draw_queries_one(jax.random.fold_in(seeds[15], 71), 0)
    queries_two = draw_queries_two(jax.random.fold_in(seeds[15], 71), 0)
    keys_one = draw_keys_one(jax.random.fold_in(seeds[15], 71), 0)
    keys_two = draw_keys_two(jax.random.fold_in(seeds[15], 71), 0)
    values = gaussian(seeds[5], (TOKENS, KV_HEADS * VAL_DIM), 1.0, 6.0, ((0, 8), (1, 4)))
    lambdas = jnp.clip(0.3 + 0.5 * jax.random.uniform(seeds[6], (HEADS,), jnp.float32) ** steps_of(seeds[6], (HEADS,), ((0, 4),), -0.2, 0.2), 0.3, 0.8)
    head_gain = jnp.clip(1.0 + 0.18 * jax.random.normal(seeds[7], (VAL_DIM,), jnp.float32), 0.1, 1.9)
    out_weight = gaussian(seeds[8], (HEADS * VAL_DIM, D), (HEADS * VAL_DIM) ** -0.5, 0.125, ((0, 4),))
    norm_gain = jnp.clip(1.0 + 0.18 * jax.random.normal(seeds[9], (D,), jnp.float32), 0.1, 1.9)
    expert_ids_keys = jax.random.split(jax.random.fold_in(seeds[10], 1), TOKENS // ROWS_DEV)
    expert_ids_turns = jax.random.permutation(jax.random.fold_in(seeds[10], 3), TOKENS // ROWS_DEV)
    expert_ids = jax.vmap(lambda own, number: deal_out(jax.random.fold_in(seeds[10], 2), own, number, ROWS_DEV, EXPERTS, TOPK, CAP, 1))(expert_ids_keys, expert_ids_turns).reshape((TOKENS, TOPK))
    route_weight = jnp.clip(0.1 + 0.9 * jax.random.uniform(seeds[11], (TOKENS, TOPK), jnp.float32) ** steps_of(seeds[11], (TOKENS, TOPK), ((0, 32),), -0.2, 0.2), 0.1, 1.0)
    gate_weight = gaussian(seeds[12], (EXPERTS, D, EXPERT_FF), D ** -0.5, 0.125, ((0, 8), (2, 4)))
    up_weight = gaussian(seeds[13], (EXPERTS, D, EXPERT_FF), D ** -0.5, 0.125, ((0, 8), (2, 4)))
    down_weight = gaussian(seeds[14], (EXPERTS, EXPERT_FF, D), EXPERT_FF ** -0.5, 0.1875, ((0, 8), (1, 4)))
    return {"stream_in": stream_in, "queries_one": queries_one, "queries_two": queries_two, "keys_one": keys_one, "keys_two": keys_two, "values": values, "lambdas": lambdas, "head_gain": head_gain, "out_weight": out_weight, "norm_gain": norm_gain, "expert_ids": expert_ids, "route_weight": route_weight, "gate_weight": gate_weight, "up_weight": up_weight, "down_weight": down_weight}


EPS = 1e-06
OUT_SCALE = 0.8

def mix_map(queries, keys, vals, allowed):
    scores = jnp.einsum('qrd,kd->rqk', queries, keys) * HEAD_DIM ** (-0.5)
    scores = jnp.where(allowed[None], scores, -jnp.inf)
    row_max = lax.optimization_barrier(jnp.max(scores, axis=-1, keepdims=True))
    exp_terms = jnp.exp(scores - row_max)
    totals = lax.optimization_barrier(jnp.sum(exp_terms, axis=-1, keepdims=True))
    weights = lax.optimization_barrier(exp_terms.astype(jnp.bfloat16)).astype(jnp.float32)
    return jnp.einsum('rqk,kv->rqv', weights, vals) / totals

def reference(stream_in, queries_one, queries_two, keys_one, keys_two, values, lambdas, head_gain, out_weight, norm_gain, expert_ids, route_weight, gate_weight, up_weight, down_weight):
    per_kv = HEADS // KV_HEADS
    q_block = math.gcd(TOKENS, 512)
    num_blocks = TOKENS // q_block
    key_pos = jnp.arange(TOKENS, dtype=jnp.int32)
    keys_first = keys_one.astype(jnp.float32)
    keys_second = keys_two.astype(jnp.float32)
    vals_all = values.astype(jnp.float32)

    def one_block(block_index):
        first_row = (block_index * q_block).astype(jnp.int32)
        q_first = lax.dynamic_slice_in_dim(queries_one, first_row, q_block, 0).astype(jnp.float32).reshape(q_block, HEADS, HEAD_DIM)
        q_second = lax.dynamic_slice_in_dim(queries_two, first_row, q_block, 0).astype(jnp.float32).reshape(q_block, HEADS, HEAD_DIM)
        query_pos = first_row + jnp.arange(q_block, dtype=jnp.int32)
        allowed = key_pos[None, :] <= query_pos[:, None]
        head_outs = []
        for kv_index in range(KV_HEADS):
            lo_head = kv_index * per_kv
            key_cols = slice(kv_index * HEAD_DIM, (kv_index + 1) * HEAD_DIM)
            val_cols = slice(kv_index * VAL_DIM, (kv_index + 1) * VAL_DIM)
            mix_first = mix_map(q_first[:, lo_head:lo_head + per_kv], keys_first[:, key_cols], vals_all[:, val_cols], allowed)
            mix_second = mix_map(q_second[:, lo_head:lo_head + per_kv], keys_second[:, key_cols], vals_all[:, val_cols], allowed)
            lambda_rows = lambdas[lo_head:lo_head + per_kv][:, None, None]
            head_outs.append(mix_first - lambda_rows * mix_second)
        difference = jnp.concatenate(head_outs, 0)
        mean_sq = lax.optimization_barrier(jnp.mean(difference * difference, axis=-1, keepdims=True))
        normed_heads = difference * lax.rsqrt(mean_sq + EPS) * head_gain * OUT_SCALE
        return normed_heads.transpose(1, 0, 2).reshape(q_block, HEADS * VAL_DIM).astype(jnp.bfloat16)
    heads_out = lax.map(one_block, jnp.arange(num_blocks, dtype=jnp.int32)).reshape(TOKENS, HEADS * VAL_DIM)
    col_width = HEADS * VAL_DIM // N_TP
    stream = stream_in.astype(jnp.float32)
    for group_no in range(N_TP):
        cols = slice(group_no * col_width, (group_no + 1) * col_width)
        partial_value = jnp.dot(heads_out[:, cols], out_weight[cols], preferred_element_type=jnp.float32)
        stream = stream + lax.optimization_barrier(partial_value.astype(jnp.bfloat16)).astype(jnp.float32)
    normed = (stream * lax.rsqrt(lax.optimization_barrier(jnp.mean(stream * stream, axis=-1, keepdims=True)) + EPS) * norm_gain).astype(jnp.bfloat16)
    flat_ids = expert_ids.reshape(-1)
    owners = jnp.arange(TOKENS * TOPK, dtype=jnp.int32) // TOPK
    rows_all = jnp.take(normed, owners, axis=0)
    capacity = N_SP * N_TP * CAP
    quarter = EXPERT_FF // N_TP

    def per_expert(collected, weights_item):
        gate_w, up_w, down_w, number = weights_item
        chosen = flat_ids == number
        places = jnp.cumsum(chosen.astype(jnp.int32)) - 1
        target = jnp.where(chosen, places, capacity).astype(jnp.int32)
        buffer = jnp.zeros((capacity + 1, D), jnp.bfloat16).at[target].set(rows_all)[:capacity]
        gate = jnp.dot(buffer, gate_w, preferred_element_type=jnp.float32)
        upper = jnp.dot(buffer, up_w, preferred_element_type=jnp.float32)
        hidden = (jax.nn.silu(gate) * upper).astype(jnp.bfloat16)
        summed = jnp.zeros((capacity, D), jnp.float32)
        for group_no in range(N_TP):
            units = slice(group_no * quarter, (group_no + 1) * quarter)
            partial_value = jnp.dot(hidden[:, units], down_w[units], preferred_element_type=jnp.float32)
            summed = summed + lax.optimization_barrier(partial_value.astype(jnp.bfloat16)).astype(jnp.float32)
        result = jnp.concatenate([summed.astype(jnp.bfloat16), jnp.zeros((1, D), jnp.bfloat16)], 0)
        collected = jnp.where(chosen[:, None], jnp.take(result, target, axis=0), collected)
        return (collected, None)
    collected, _ = lax.scan(per_expert, jnp.zeros((TOKENS * TOPK, D), jnp.bfloat16), (gate_weight, up_weight, down_weight, jnp.arange(EXPERTS, dtype=jnp.int32)))
    routed = lax.optimization_barrier(jnp.sum(collected.reshape(TOKENS, TOPK, D).astype(jnp.float32) * route_weight[:, :, None], axis=1))
    return (stream + routed).astype(jnp.bfloat16)
```

```python
import functools

import jax
import jax.numpy as jnp
from jax import lax
from jax.experimental import pallas as pl
from jax.experimental.pallas import tpu as pltpu
from jax.sharding import PartitionSpec as P

HEAD_DIM = 128
VAL_DIM = 256


EPS = 1e-06
OUT_SCALE = 0.8


MESH = pl.DeviceIdType.MESH
LOG2E = 1.4426950408889634
DEEP = 8
WIDE = 8
DOWN = ((0, 2), (2, 2), (4, 2), (6, 1), (7, 1))
PARTS = 4


def remote(src, dst, send_sem, recv_sem, where):
    return pltpu.make_async_remote_copy(
        src_ref=src,
        dst_ref=dst,
        send_sem=send_sem,
        recv_sem=recv_sem,
        device_id=where,
        device_id_type=MESH,
    )


def greet(devices, count):
    barrier = pltpu.get_barrier_semaphore()
    devices(lambda where: pl.semaphore_signal(barrier, inc=1, device_id=where, device_id_type=MESH))
    pl.semaphore_wait(barrier, count)


def layer_kernel(n, nt, cap, *refs):
    (
        q1_ref, q2_ref, k1_ref, k2_ref, v_ref, lam_ref, gain_ref, ow_ref, stream_ref, norm_ref,
    ) = refs[:10]
    if cap:
        ids_ref, route_ref, gw_ref, uw_ref, dw_ref, out_ref = refs[10:16]
        refs = refs[16:]
    else:
        stream_out, normed_out = refs[10:12]
        refs = refs[12:]
    kv, qs, top, total, acc, heads, ow, near_part, near_got, far_part, far_got = refs[:11]
    local_sem, z_send, z_recv, y_send, y_recv, p_send, p_recv = refs[11:18]
    if cap:
        (
            stream_out, normed_out, gu, dw, blend, blend_hi, blend_lo, send, rows_in, hid, ret, back,
            own_sem, w_send, w_recv, f_send, f_recv, g_send, g_recv, d_send, d_recv, r_send, r_recv,
        ) = refs[18:]

    me, tp = lax.axis_index("sp"), lax.axis_index("tp")
    nz = n // 2
    zi, y = me // 2, lax.rem(me, 2)
    pair = me + 1 - 2 * y
    rows = q1_ref.shape[0]
    hd = HEAD_DIM
    chunk = rows // nt
    side, core = tp // 2, lax.rem(tp, 2)
    near = (me, tp + 1 - 2 * core)
    far = (me, lax.rem(tp + 2, 4))

    loads = [
        pltpu.make_async_copy(k1_ref, kv.at[me, :, pl.ds(0, hd)], local_sem.at[0]),
        pltpu.make_async_copy(k2_ref, kv.at[me, :, pl.ds(hd, hd)], local_sem.at[1]),
        pltpu.make_async_copy(v_ref, kv.at[me, :, pl.ds(2 * hd, VAL_DIM)], local_sem.at[2]),
    ]
    for load in loads:
        load.start()
    if cap:
        ff = gw_ref.shape[2]

        deep = gu.shape[1] // DEEP
        wide = dw.shape[1] // WIDE

        def part_of(i, k):
            if i == 2:
                return dw.at[pl.ds(k * ff, ff), :]
            return gu.at[i, :, pl.ds(k * ff, ff)]

        own_loads = [
            pltpu.make_async_copy(ref.at[0], part_of(i, 0), own_sem.at[i])
            for i, ref in enumerate((gw_ref, uw_ref, dw_ref))
        ]
        for load in own_loads:
            load.start()

        def w_copy(i):
            return remote(part_of(i, 0), part_of(i, 1), w_send.at[i], w_recv.at[i], near)

        def piece(p, k):
            rows_of = pl.ds(pl.multiple_of(lax.rem(p, DEEP) * deep, deep), deep)
            return gu.at[p // DEEP, rows_of, pl.ds(k * ff, ff)]

        def far_piece(p):
            return remote(piece(p, 0), piece(p, 2), f_send.at[p], f_recv.at[p], far)

        def relay(p):
            return remote(piece(p, 2), piece(p, 3), g_send.at[p], g_recv.at[p], near)

        def down_piece(j, k):
            first, count = DOWN[j]
            return dw.at[pl.ds(k * ff, ff), pl.ds(first * wide, count * wide)]

        def far_down(j):
            p = 2 * DEEP + j
            return remote(down_piece(j, 0), down_piece(j, 2), f_send.at[p], f_recv.at[p], far)

        def relay_down(j):
            p = 2 * DEEP + j
            return remote(down_piece(j, 2), down_piece(j, 3), g_send.at[p], g_recv.at[p], near)

        ahead = jnp.where(zi == 0, 1, jnp.minimum(3 + 2 * zi, 2 * DEEP))

        def far_some(p, _):
            far_piece(p).start()
            return 0

    ow_load = pltpu.make_async_copy(ow_ref, ow, local_sem.at[3])
    ow_load.start()

    def peers(tell):
        def column(s, _):
            @pl.when(s != me)
            def _():
                tell((s, tp))
            return 0
        lax.fori_loop(0, n, column, 0)
        tell(near)
        tell(far)

    greet(peers, n - 1 + 2)
    for load in loads:
        load.wait()

    def hop(z):
        b = 2 * z + y
        return remote(kv.at[b], kv.at[b], z_send.at[z], z_recv.at[z], (lax.rem(me + 2, n), tp))

    def y_copy(z):
        b = 2 * z + y
        return remote(kv.at[b], kv.at[b], y_send.at[z], y_recv.at[z], (pair, tp))

    def y_arrival(z):
        b = 2 * z + 1 - y
        return remote(kv.at[b], kv.at[b], y_send.at[z], y_recv.at[z], (pair, tp))

    @pl.when(zi < nz - 1)
    def _():
        hop(zi).start()

    @pl.when(y == 0)
    def _():
        y_copy(zi).start()

    if cap:
        own_loads[0].wait()
        own_loads[1].wait()
        lax.fori_loop(0, ahead, far_some, 0)
        own_loads[2].wait()
        for i in range(3):
            w_copy(i).start()

    for i, ref in enumerate((q1_ref, q2_ref)):
        for h in range(2):
            qs[i, h * rows:(h + 1) * rows, :] = ref[:, h * hd:(h + 1) * hd]

    scale = HEAD_DIM ** (-0.5) * LOG2E

    def fold(b, first):
        vals = kv[b, :, 2 * hd:]
        for i in range(2):
            keys = kv[b, :, i * hd:(i + 1) * hd]
            s = lax.dot_general(qs[i], keys, (((1,), (1,)), ((), ())), preferred_element_type=jnp.float32)
            if first:
                r = lax.broadcasted_iota(jnp.int32, (2, rows, rows), 1).reshape(2 * rows, rows)
                c = lax.broadcasted_iota(jnp.int32, (2 * rows, rows), 1)
                s = jnp.where(c <= r, s, -jnp.inf)
                new = jnp.max(s, axis=-1, keepdims=True)
            else:
                old = top[i][:, :1]
                new = jnp.maximum(old, jnp.max(s, axis=-1, keepdims=True))
            e = jnp.exp2((s - new) * scale)
            part = sum(e[:, c * 128:(c + 1) * 128] for c in range(rows // 128))
            pv = jnp.dot(e.astype(jnp.bfloat16), vals, preferred_element_type=jnp.float32)
            if first:
                acc[i] = pv
                total[i] = part
            else:
                alpha = jnp.exp2((old - new) * scale)
                acc[i] = acc[i] * alpha + pv
                total[i] = total[i] * alpha + part
            top[i] = jnp.broadcast_to(new, (2 * rows, 128))

    fold(me, True)

    if cap:
        choices, tokens = ids_ref.shape
        which = lax.broadcasted_iota(jnp.int32, (max(n, 8), tokens), 0)
        named = [(ids_ref[k:k + 1, :] == which).astype(jnp.float32) for k in range(choices)]
        before = lax.broadcasted_iota(jnp.int32, (tokens, tokens), 0) < lax.broadcasted_iota(
            jnp.int32, (tokens, tokens), 1
        )
        counts = jnp.dot(
            sum(named).astype(jnp.bfloat16), before.astype(jnp.bfloat16), preferred_element_type=jnp.float32
        )
        place = lax.broadcasted_iota(jnp.int32, (n * cap, tokens), 0)
        chosen = jnp.zeros((n * cap, tokens), jnp.float32)
        weight = jnp.zeros((n * cap, tokens), jnp.float32)
        for k in range(choices):
            rank = jnp.sum(named[k] * counts, axis=0, keepdims=True).astype(jnp.int32)
            hit = (ids_ref[k:k + 1, :] * cap + rank) == place
            chosen = chosen + hit.astype(jnp.float32)
            weight = weight + jnp.where(hit, route_ref[k:k + 1, :], 0.0)
        blend[...] = chosen.astype(jnp.bfloat16)
        weight = weight.T
        coarse = weight.astype(jnp.bfloat16)
        blend_hi[...] = coarse
        blend_lo[...] = (weight - coarse.astype(jnp.float32)).astype(jnp.bfloat16)

    @pl.when(y == 1)
    def _():
        y_arrival(zi).wait_recv()
        fold(pair, False)

    def walk(d, _):
        z = zi - d
        @pl.when(d <= zi)
        def _():
            hop(z).wait_recv()
            y_copy(z).start()
            @pl.when(zi < nz - 1)
            def _():
                hop(z).start()
            fold(2 * z + y, False)
        @pl.when(d > 1)
        def _():
            y_arrival(z + 1).wait_recv()
            fold(2 * (z + 1) + 1 - y, False)
        return 0

    lax.fori_loop(1, jnp.where(zi > 0, zi + 2, 1), walk, 0)

    for h in range(2):
        r = pl.ds(h * rows, rows)
        one = acc[0, r, :] / jnp.sum(total[0, r, :], axis=-1, keepdims=True)
        two = acc[1, r, :] / jnp.sum(total[1, r, :], axis=-1, keepdims=True)
        diff = one - lam_ref[h] * two
        ms = jnp.mean(diff * diff, axis=-1, keepdims=True)
        heads[:, h * VAL_DIM:(h + 1) * VAL_DIM] = (
            diff * lax.rsqrt(ms + EPS) * gain_ref[...] * OUT_SCALE
        ).astype(jnp.bfloat16)

    ow_load.wait()

    d_model = ow.shape[1]
    span = d_model // PARTS

    def picked(first, second):
        return jnp.concatenate(
            [heads[pl.ds(pl.multiple_of(t * chunk, chunk), chunk), :] for t in (first, second)], axis=0
        )

    def near_copy(q):
        cols = pl.ds(q * span, span)
        return remote(near_part.at[:, cols], near_got.at[:, cols], p_send.at[0, q], p_recv.at[0, q], near)

    def far_copy(q):
        cols = pl.ds(q * span, span)
        return remote(far_part.at[:, cols], far_got.at[:, cols], p_send.at[1, q], p_recv.at[1, q], far)

    away = 1 - side
    other = picked(2 * away + 1 - core, 2 * side + 1 - core)
    for q in range(PARTS):
        cols = slice(q * span, (q + 1) * span)
        near_part[:, cols] = jnp.dot(
            other, ow[:, cols], preferred_element_type=jnp.float32
        ).astype(jnp.bfloat16)
        near_copy(q).start()
    own = picked(2 * away + core, 2 * side + core)
    for q in range(PARTS):
        cols = slice(q * span, (q + 1) * span)
        mine = jnp.dot(own, ow[:, cols], preferred_element_type=jnp.float32)
        near_copy(q).wait_recv()
        mine = mine + near_got[:, cols].astype(jnp.float32)
        far_part[:, cols] = mine[:chunk].astype(jnp.bfloat16)
        far_copy(q).start()
        stream_out[:, cols] = stream_ref[:, cols].astype(jnp.float32) + mine[chunk:]
    if cap:
        lax.fori_loop(ahead, 2 * DEEP, far_some, 0)
        for j in range(len(DOWN)):
            far_down(j).start()
    square = jnp.zeros((chunk, 1), jnp.float32)
    for q in range(PARTS):
        cols = slice(q * span, (q + 1) * span)
        far_copy(q).wait_recv()
        summed = stream_out[:, cols] + far_got[:, cols].astype(jnp.float32)
        stream_out[:, cols] = summed
        square = square + jnp.sum(summed * summed, axis=-1, keepdims=True)
    normed_out[...] = (
        stream_out[...] * lax.rsqrt(square * (1.0 / d_model) + EPS) * norm_ref[...]
    ).astype(jnp.bfloat16)

    def finish_attention():
        for q in range(PARTS):
            near_copy(q).wait_send()
            far_copy(q).wait_send()

        @pl.when(y == 0)
        def _():
            y_copy(zi).wait_send()

        @pl.when(zi < nz - 1)
        def _():
            hop(zi).wait_send()

        def sent(z, _):
            y_copy(z).wait_send()
            @pl.when(zi < nz - 1)
            def _():
                hop(z).wait_send()
            return 0

        lax.fori_loop(0, zi, sent, 0)

    if not cap:
        finish_attention()
        return

    def d_copy(s):
        return remote(send.at[s], rows_in.at[me], d_send.at[s], d_recv.at[me], (s, tp))

    def d_arrival(s):
        return remote(send.at[s], rows_in.at[s], d_send.at[s], d_recv.at[s], (s, tp))

    def r_copy(j, s):
        first, count = DOWN[j]
        w = pl.ds(first, count)
        return remote(ret.at[w, s], back.at[w, me], r_send.at[j, s], r_recv.at[j, me], (s, tp))

    def r_arrival(j, s):
        first, count = DOWN[j]
        w = pl.ds(first, count)
        return remote(ret.at[w, s], back.at[w, s], r_send.at[j, s], r_recv.at[j, s], (s, tp))

    def dispatch(d, _):
        z = lax.rem(zi + d, nz)
        base = pl.multiple_of(2 * z * cap, 2 * cap)
        got = jnp.dot(
            blend[pl.ds(base, 2 * cap), :], normed_out[...], preferred_element_type=jnp.float32
        ).astype(jnp.bfloat16)
        for j in range(2):
            s = 2 * z + j
            @pl.when(s != me)
            def _():
                send[s] = got[j * cap:(j + 1) * cap]
                d_copy(s).start()
            @pl.when(s == me)
            def _():
                rows_in[me] = got[j * cap:(j + 1) * cap]
        return 0

    lax.fori_loop(1, nz + 1, dispatch, 0)

    def pass_on(p, _):
        far_piece(p).wait_recv()
        relay(p).start()
        return 0

    lax.fori_loop(0, DEEP, pass_on, 0)
    for i in range(3):
        w_copy(i).wait_recv()
    local = 2 * ff

    def gated(x, cols):
        gate = jnp.dot(x, gu[0, :, cols], preferred_element_type=jnp.float32)
        upper = jnp.dot(x, gu[1, :, cols], preferred_element_type=jnp.float32)
        return (gate / (1.0 + jnp.exp(-gate)) * upper).astype(jnp.bfloat16)

    def work(z, _):
        lax.fori_loop(DEEP + z * (DEEP // nz), DEEP + (z + 1) * (DEEP // nz), pass_on, 0)
        for j in range(2):
            s = 2 * z + j
            @pl.when(s != me)
            def _():
                d_arrival(s).wait_recv()
        x = rows_in[pl.ds(2 * z, 2)].reshape(2 * cap, d_model)
        base = pl.multiple_of(2 * z * cap, 2 * cap)
        hid[pl.ds(base, 2 * cap), :local] = gated(x, slice(0, local))
        return 0

    lax.fori_loop(0, nz, work, 0)

    def relayed(p, _):
        relay(p).wait_recv()
        return 0

    lax.fori_loop(0, 2 * DEEP, relayed, 0)
    hid[:, local:] = gated(rows_in[...].reshape(n * cap, d_model), slice(local, 2 * local))

    def give_back(j):
        far_down(j).wait_recv()
        relay_down(j).start()
        relay_down(j).wait_recv()
        first, count = DOWN[j]
        down = jnp.dot(
            hid[...], dw[:, first * wide:(first + count) * wide], preferred_element_type=jnp.float32
        ).astype(jnp.bfloat16)
        for c in range(count):
            ret[first + c] = down[:, c * wide:(c + 1) * wide].reshape(n, cap, wide)
            back[first + c, me] = ret[first + c, me]

        def one(d, _):
            for k in range(2):
                s = 2 * lax.rem(zi + d, nz) + k
                @pl.when(s != me)
                def _():
                    r_copy(j, s).start()
            return 0

        lax.fori_loop(1, nz + 1, one, 0)

    def collect(j):
        def arrive(s, _):
            @pl.when(s != me)
            def _():
                r_arrival(j, s).wait_recv()
            return 0

        lax.fori_loop(0, n, arrive, 0)
        first, count = DOWN[j]
        for c in range(first, first + count):
            results = back[c].reshape(n * cap, wide)
            routed = jnp.dot(blend_hi[...], results, preferred_element_type=jnp.float32)
            routed = routed + jnp.dot(blend_lo[...], results, preferred_element_type=jnp.float32)
            cols = slice(c * wide, (c + 1) * wide)
            out_ref[:, cols] = (stream_out[:, cols] + routed).astype(jnp.bfloat16)

    for j in range(len(DOWN)):
        give_back(j)
        if j > 1:
            collect(j - 2)
    for j in range(max(len(DOWN) - 2, 0), len(DOWN)):
        collect(j)

    finish_attention()
    for i in range(3):
        w_copy(i).wait_send()

    def passed(p, _):
        far_piece(p).wait_send()
        relay(p).wait_send()
        return 0

    lax.fori_loop(0, 2 * DEEP, passed, 0)
    for j in range(len(DOWN)):
        far_down(j).wait_send()
        relay_down(j).wait_send()

    def finish(s, _):
        @pl.when(s != me)
        def _():
            d_copy(s).wait_send()
            for j in range(len(DOWN)):
                r_copy(j, s).wait_send()
        return 0

    lax.fori_loop(0, n, finish, 0)


def layer(n, nt, cap, *args):
    q1, ow, stream_in = args[0], args[7], args[8]
    rows = q1.shape[0]
    tokens, d = stream_in.shape
    vm = pl.BlockSpec(memory_space=pltpu.VMEM)
    hbm = pl.BlockSpec(memory_space=pl.ANY)
    sm = pl.BlockSpec(memory_space=pltpu.SMEM)
    chunk = rows // nt
    dma = pltpu.SemaphoreType.DMA
    bf, f32 = jnp.bfloat16, jnp.float32
    in_specs = [vm, vm, hbm, hbm, hbm, sm, vm, hbm, vm, vm]
    out_shape = (jax.ShapeDtypeStruct((tokens, d), f32), jax.ShapeDtypeStruct((tokens, d), bf))
    out_specs = (vm, vm)
    scratch = [
        pltpu.VMEM((n, rows, 2 * HEAD_DIM + VAL_DIM), bf),
        pltpu.VMEM((2, 2 * rows, HEAD_DIM), bf),
        pltpu.VMEM((2, 2 * rows, 128), f32),
        pltpu.VMEM((2, 2 * rows, 128), f32),
        pltpu.VMEM((2, 2 * rows, VAL_DIM), f32),
        pltpu.VMEM((rows, 2 * VAL_DIM), bf),
        pltpu.VMEM(ow.shape, bf),
        pltpu.VMEM((2 * chunk, d), bf),
        pltpu.VMEM((2 * chunk, d), bf),
        pltpu.VMEM((chunk, d), bf),
        pltpu.VMEM((chunk, d), bf),
        dma((4,)), dma((n // 2,)), dma((n // 2,)), dma((n // 2,)), dma((n // 2,)), dma((2, PARTS)), dma((2, PARTS)),
    ]
    if cap:
        ff = args[12].shape[2]
        in_specs = in_specs + [vm, vm, hbm, hbm, hbm]
        out_shape = jax.ShapeDtypeStruct((tokens, d), bf)
        out_specs = vm
        scratch = scratch + [
            pltpu.VMEM((tokens, d), f32),
            pltpu.VMEM((tokens, d), bf),
            pltpu.VMEM((2, d, nt * ff), bf),
            pltpu.VMEM((nt * ff, d), bf),
            pltpu.VMEM((n * cap, tokens), bf),
            pltpu.VMEM((tokens, n * cap), bf),
            pltpu.VMEM((tokens, n * cap), bf),
        ] + [pltpu.VMEM((n, cap, d), bf)] * 2 + [
            pltpu.VMEM((n * cap, nt * ff), bf),
            pltpu.VMEM((WIDE, n, cap, d // WIDE), bf),
            pltpu.VMEM((WIDE, n, cap, d // WIDE), bf),
            dma((3,)), dma((3,)), dma((3,)),
        ] + [dma((2 * DEEP + len(DOWN),))] * 4 + [dma((n,))] * 2 + [dma((len(DOWN), n))] * 2
    return pl.pallas_call(
        functools.partial(layer_kernel, n, nt, cap),
        out_shape=out_shape,
        in_specs=in_specs,
        out_specs=out_specs,
        scratch_shapes=scratch,
        compiler_params=pltpu.CompilerParams(
            collective_id=0, has_side_effects=True, vmem_limit_bytes=58 * 2**20
        ),
        name="layer",
    )(*args)


def shards(
    stream_in,
    queries_one,
    queries_two,
    keys_one,
    keys_two,
    values,
    lambdas,
    head_gain,
    out_weight,
    norm_gain,
    expert_ids,
    route_weight,
    gate_weight,
    up_weight,
    down_weight,
):
    n, nt = lax.axis_size("sp"), lax.axis_size("tp")
    rows_here = stream_in.shape[0]
    top_count = expert_ids.shape[1]
    slot_cap = 2 * top_count * rows_here // n
    shared = (
        queries_one, queries_two, keys_one, keys_two, values, lambdas,
        head_gain.reshape(1, -1), out_weight, stream_in, norm_gain.reshape(1, -1),
    )
    if slot_cap % 16 == 0:
        return layer(
            n, nt, slot_cap, *shared, expert_ids.T, route_weight.T, gate_weight, up_weight, down_weight
        )
    stream, normed = layer(n, nt, 0, *shared)
    flat_ids = expert_ids.reshape(-1)
    count = flat_ids.shape[0]
    order = lax.iota(jnp.int32, count)
    earlier = (flat_ids[None, :] == flat_ids[:, None]) & (order[None, :] < order[:, None])
    ranks = jnp.sum(earlier.astype(jnp.int32), axis=1)
    slots = flat_ids * slot_cap + ranks
    slot_of = slots.reshape(rows_here, top_count)
    places = lax.iota(jnp.int32, n * slot_cap)
    selector = sum(
        (slot_of[:, k][None, :] == places[:, None]).astype(jnp.bfloat16) for k in range(top_count)
    )
    send_rows = jnp.dot(selector, normed, preferred_element_type=jnp.float32).astype(jnp.bfloat16)
    received = lax.all_to_all(send_rows, "sp", split_axis=0, concat_axis=0, tiled=True)
    picked_rows = lax.all_gather(received, "tp", axis=0, tiled=True)
    gate = jnp.dot(picked_rows, gate_weight[0], preferred_element_type=jnp.float32)
    upper = jnp.dot(picked_rows, up_weight[0], preferred_element_type=jnp.float32)
    hidden = (jax.nn.silu(gate) * upper).astype(jnp.bfloat16)
    summed = lax.psum_scatter(
        jnp.dot(hidden, down_weight[0], preferred_element_type=jnp.float32).astype(jnp.bfloat16),
        "tp",
        scatter_dimension=0,
        tiled=True,
    )
    returned = lax.all_to_all(summed, "sp", split_axis=0, concat_axis=0, tiled=True)
    picked = jnp.take(returned, slots, axis=0).reshape(rows_here, top_count, -1).astype(jnp.float32)
    routed = jnp.sum(picked * route_weight[:, :, None], axis=1)
    return (stream + routed).astype(jnp.bfloat16)


def solution(mesh):
    return jax.shard_map(
        shards,
        mesh=mesh,
        in_specs=(
            P(("sp", "tp"), None),
            P("sp", "tp"),
            P("sp", "tp"),
            P("sp", "tp"),
            P("sp", "tp"),
            P("sp", "tp"),
            P("tp"),
            P(),
            P("tp", None),
            P(),
            P(("sp", "tp"), None),
            P(("sp", "tp"), None),
            P("sp", None, "tp"),
            P("sp", None, "tp"),
            P("sp", "tp", None),
        ),
        out_specs=P(("sp", "tp"), None),
        check_vma=False,
    )
```

```python
import functools

import jax
import jax.numpy as jnp
from jax import lax
from jax.experimental import pallas as pl
from jax.experimental.pallas import tpu as pltpu
from jax.sharding import PartitionSpec as P

HEAD_DIM = 128
VAL_DIM = 256


EPS = 1e-06
OUT_SCALE = 0.8


MESH = pl.DeviceIdType.MESH
LOG2E = 1.4426950408889634
PIECES = 8
PARTS = 4


def remote(src, dst, send_sem, recv_sem, where):
    return pltpu.make_async_remote_copy(
        src_ref=src,
        dst_ref=dst,
        send_sem=send_sem,
        recv_sem=recv_sem,
        device_id=where,
        device_id_type=MESH,
    )


def greet(devices, count):
    barrier = pltpu.get_barrier_semaphore()
    devices(lambda where: pl.semaphore_signal(barrier, inc=1, device_id=where, device_id_type=MESH))
    pl.semaphore_wait(barrier, count)


def layer_kernel(n, nt, cap, *refs):
    (
        q1_ref, q2_ref, k1_ref, k2_ref, v_ref, lam_ref, gain_ref, ow_ref, stream_ref, norm_ref,
    ) = refs[:10]
    if cap:
        ids_ref, route_ref, gw_ref, uw_ref, dw_ref, out_ref = refs[10:16]
        refs = refs[16:]
    else:
        stream_out, normed_out = refs[10:12]
        refs = refs[12:]
    kv, qs, top, total, acc, heads, ow, near_part, near_got, far_part, far_got = refs[:11]
    local_sem, z_send, z_recv, y_send, y_recv, p_send, p_recv = refs[11:18]
    if cap:
        (
            stream_out, normed_out, gu, dw, blend, blend_hi, blend_lo, send, rows_in, hid_out, hid_in, ret, back,
            own_sem, w_send, w_recv, f_send, f_recv, g_send, g_recv, d_send, d_recv,
            a_send, a_recv, h_send, h_recv, r_send, r_recv,
        ) = refs[18:]

    me, tp = lax.axis_index("sp"), lax.axis_index("tp")
    nz = n // 2
    zi, y = me // 2, lax.rem(me, 2)
    pair = me + 1 - 2 * y
    rows = q1_ref.shape[0]
    hd = HEAD_DIM
    chunk = rows // nt
    side, core = tp // 2, lax.rem(tp, 2)
    near = (me, tp + 1 - 2 * core)
    far = (me, lax.rem(tp + 2, 4))
    cross = (me, 3 - tp)

    loads = [
        pltpu.make_async_copy(k1_ref, kv.at[me, :, pl.ds(0, hd)], local_sem.at[0]),
        pltpu.make_async_copy(k2_ref, kv.at[me, :, pl.ds(hd, hd)], local_sem.at[1]),
        pltpu.make_async_copy(v_ref, kv.at[me, :, pl.ds(2 * hd, VAL_DIM)], local_sem.at[2]),
    ]
    for load in loads:
        load.start()
    if cap:
        ff = gw_ref.shape[2]

        deep = ff // PIECES
        own_loads = [
            pltpu.make_async_copy(dw_ref.at[0], dw.at[pl.ds(0, ff), :], own_sem.at[0]),
            pltpu.make_async_copy(gw_ref.at[0], gu.at[:, pl.ds(0, ff)], own_sem.at[1]),
            pltpu.make_async_copy(uw_ref.at[0], gu.at[:, pl.ds(ff, ff)], own_sem.at[2]),
        ]
        for load in own_loads:
            load.start()
        w_copy = remote(dw.at[pl.ds(0, ff), :], dw.at[pl.ds(ff, ff), :], w_send.at[0], w_recv.at[0], near)

        def piece(p, k):
            return dw.at[pl.ds(pl.multiple_of(k * ff + p * deep, deep), deep), :]

        def far_piece(p):
            return remote(piece(p, 0), piece(p, 2), f_send.at[p], f_recv.at[p], far)

        def relay(p):
            return remote(piece(p, 2), piece(p, 3), g_send.at[p], g_recv.at[p], near)

        ahead = jnp.minimum(3 + 3 * zi, PIECES)

        def far_some(p, _):
            far_piece(p).start()
            return 0

    ow_load = pltpu.make_async_copy(ow_ref, ow, local_sem.at[3])
    ow_load.start()

    def peers(tell):
        def column(s, _):
            @pl.when(s != me)
            def _():
                tell((s, tp))
            return 0
        lax.fori_loop(0, n, column, 0)
        tell(near)
        tell(far)
        tell(cross)

    greet(peers, n - 1 + 3)
    for load in loads:
        load.wait()

    def hop(z):
        b = 2 * z + y
        return remote(kv.at[b], kv.at[b], z_send.at[z], z_recv.at[z], (lax.rem(me + 2, n), tp))

    def y_copy(z):
        b = 2 * z + y
        return remote(kv.at[b], kv.at[b], y_send.at[z], y_recv.at[z], (pair, tp))

    def y_arrival(z):
        b = 2 * z + 1 - y
        return remote(kv.at[b], kv.at[b], y_send.at[z], y_recv.at[z], (pair, tp))

    @pl.when(zi < nz - 1)
    def _():
        hop(zi).start()

    @pl.when(y == 0)
    def _():
        y_copy(zi).start()

    if cap:
        own_loads[0].wait()
        lax.fori_loop(0, ahead, far_some, 0)
        w_copy.start()

    for i, ref in enumerate((q1_ref, q2_ref)):
        for h in range(2):
            qs[i, h * rows:(h + 1) * rows, :] = ref[:, h * hd:(h + 1) * hd]

    scale = HEAD_DIM ** (-0.5) * LOG2E

    def fold(b, first):
        vals = kv[b, :, 2 * hd:]
        for i in range(2):
            keys = kv[b, :, i * hd:(i + 1) * hd]
            s = lax.dot_general(qs[i], keys, (((1,), (1,)), ((), ())), preferred_element_type=jnp.float32)
            if first:
                r = lax.broadcasted_iota(jnp.int32, (2, rows, rows), 1).reshape(2 * rows, rows)
                c = lax.broadcasted_iota(jnp.int32, (2 * rows, rows), 1)
                s = jnp.where(c <= r, s, -jnp.inf)
                new = jnp.max(s, axis=-1, keepdims=True)
            else:
                old = top[i][:, :1]
                new = jnp.maximum(old, jnp.max(s, axis=-1, keepdims=True))
            e = jnp.exp2((s - new) * scale)
            part = sum(e[:, c * 128:(c + 1) * 128] for c in range(rows // 128))
            pv = jnp.dot(e.astype(jnp.bfloat16), vals, preferred_element_type=jnp.float32)
            if first:
                acc[i] = pv
                total[i] = part
            else:
                alpha = jnp.exp2((old - new) * scale)
                acc[i] = acc[i] * alpha + pv
                total[i] = total[i] * alpha + part
            top[i] = jnp.broadcast_to(new, (2 * rows, 128))

    fold(me, True)

    if cap:
        choices, tokens = ids_ref.shape
        which = lax.broadcasted_iota(jnp.int32, (max(n, 8), tokens), 0)
        named = [(ids_ref[k:k + 1, :] == which).astype(jnp.float32) for k in range(choices)]
        before = lax.broadcasted_iota(jnp.int32, (tokens, tokens), 0) < lax.broadcasted_iota(
            jnp.int32, (tokens, tokens), 1
        )
        counts = jnp.dot(
            sum(named).astype(jnp.bfloat16), before.astype(jnp.bfloat16), preferred_element_type=jnp.float32
        )
        place = lax.broadcasted_iota(jnp.int32, (n * cap, tokens), 0)
        chosen = jnp.zeros((n * cap, tokens), jnp.float32)
        weight = jnp.zeros((n * cap, tokens), jnp.float32)
        for k in range(choices):
            rank = jnp.sum(named[k] * counts, axis=0, keepdims=True).astype(jnp.int32)
            hit = (ids_ref[k:k + 1, :] * cap + rank) == place
            chosen = chosen + hit.astype(jnp.float32)
            weight = weight + jnp.where(hit, route_ref[k:k + 1, :], 0.0)
        blend[...] = chosen.astype(jnp.bfloat16)
        weight = weight.T
        coarse = weight.astype(jnp.bfloat16)
        blend_hi[...] = coarse
        blend_lo[...] = (weight - coarse.astype(jnp.float32)).astype(jnp.bfloat16)

    @pl.when(y == 1)
    def _():
        y_arrival(zi).wait_recv()
        fold(pair, False)

    def walk(d, _):
        z = zi - d
        @pl.when(d <= zi)
        def _():
            hop(z).wait_recv()
            y_copy(z).start()
            @pl.when(zi < nz - 1)
            def _():
                hop(z).start()
            fold(2 * z + y, False)
        @pl.when(d > 1)
        def _():
            y_arrival(z + 1).wait_recv()
            fold(2 * (z + 1) + 1 - y, False)
        return 0

    lax.fori_loop(1, jnp.where(zi > 0, zi + 2, 1), walk, 0)

    for h in range(2):
        r = pl.ds(h * rows, rows)
        one = acc[0, r, :] / jnp.sum(total[0, r, :], axis=-1, keepdims=True)
        two = acc[1, r, :] / jnp.sum(total[1, r, :], axis=-1, keepdims=True)
        diff = one - lam_ref[h] * two
        ms = jnp.mean(diff * diff, axis=-1, keepdims=True)
        heads[:, h * VAL_DIM:(h + 1) * VAL_DIM] = (
            diff * lax.rsqrt(ms + EPS) * gain_ref[...] * OUT_SCALE
        ).astype(jnp.bfloat16)

    ow_load.wait()

    d_model = ow.shape[1]
    span = d_model // PARTS

    def picked(first, second):
        return jnp.concatenate(
            [heads[pl.ds(pl.multiple_of(t * chunk, chunk), chunk), :] for t in (first, second)], axis=0
        )

    def near_copy(q):
        cols = pl.ds(q * span, span)
        return remote(near_part.at[:, cols], near_got.at[:, cols], p_send.at[0, q], p_recv.at[0, q], near)

    def far_copy(q):
        cols = pl.ds(q * span, span)
        return remote(far_part.at[:, cols], far_got.at[:, cols], p_send.at[1, q], p_recv.at[1, q], far)

    away = 1 - side
    other = picked(2 * away + 1 - core, 2 * side + 1 - core)
    for q in range(PARTS):
        cols = slice(q * span, (q + 1) * span)
        near_part[:, cols] = jnp.dot(
            other, ow[:, cols], preferred_element_type=jnp.float32
        ).astype(jnp.bfloat16)
        near_copy(q).start()
    own = picked(2 * away + core, 2 * side + core)
    for q in range(PARTS):
        cols = slice(q * span, (q + 1) * span)
        mine = jnp.dot(own, ow[:, cols], preferred_element_type=jnp.float32)
        near_copy(q).wait_recv()
        mine = mine + near_got[:, cols].astype(jnp.float32)
        far_part[:, cols] = mine[:chunk].astype(jnp.bfloat16)
        far_copy(q).start()
        stream_out[:, cols] = stream_ref[:, cols].astype(jnp.float32) + mine[chunk:]
    if cap:
        lax.fori_loop(ahead, PIECES, far_some, 0)
    square = jnp.zeros((chunk, 1), jnp.float32)
    for q in range(PARTS):
        cols = slice(q * span, (q + 1) * span)
        far_copy(q).wait_recv()
        summed = stream_out[:, cols] + far_got[:, cols].astype(jnp.float32)
        stream_out[:, cols] = summed
        square = square + jnp.sum(summed * summed, axis=-1, keepdims=True)
    normed_out[...] = (
        stream_out[...] * lax.rsqrt(square * (1.0 / d_model) + EPS) * norm_ref[...]
    ).astype(jnp.bfloat16)

    def finish_attention():
        for q in range(PARTS):
            near_copy(q).wait_send()
            far_copy(q).wait_send()

        @pl.when(y == 0)
        def _():
            y_copy(zi).wait_send()

        @pl.when(zi < nz - 1)
        def _():
            hop(zi).wait_send()

        def sent(z, _):
            y_copy(z).wait_send()
            @pl.when(zi < nz - 1)
            def _():
                hop(z).wait_send()
            return 0

        lax.fori_loop(0, zi, sent, 0)

    if not cap:
        finish_attention()
        return

    def d_copy(s):
        return remote(send.at[s], rows_in.at[0, me], d_send.at[s], d_recv.at[me], (s, tp))

    def d_arrival(s):
        return remote(send.at[s], rows_in.at[0, s], d_send.at[s], d_recv.at[s], (s, tp))

    def near_rows(s):
        return remote(rows_in.at[0, s], rows_in.at[1, s], a_send.at[0, s], a_recv.at[0, s], near)

    def far_rows(s):
        return remote(rows_in.at[0, s], rows_in.at[2, s], a_send.at[1, s], a_recv.at[1, s], far)

    def relay_rows(s):
        return remote(rows_in.at[2, s], rows_in.at[3, s], a_send.at[2, s], a_recv.at[2, s], near)

    def h_copy(z, k):
        return remote(
            hid_out.at[z, k - 1],
            hid_in.at[z, :, pl.ds(k * ff, ff)],
            h_send.at[k - 1, z],
            h_recv.at[k - 1, z],
            (near, far, cross)[k - 1],
        )

    def r_copy(s):
        return remote(ret.at[s], back.at[me], r_send.at[s], r_recv.at[me], (s, tp))

    def r_arrival(s):
        return remote(ret.at[s], back.at[s], r_send.at[s], r_recv.at[s], (s, tp))

    def dispatch(d, _):
        z = lax.rem(zi + d, nz)
        base = pl.multiple_of(2 * z * cap, 2 * cap)
        got = jnp.dot(
            blend[pl.ds(base, 2 * cap), :], normed_out[...], preferred_element_type=jnp.float32
        ).astype(jnp.bfloat16)
        for j in range(2):
            s = 2 * z + j
            @pl.when(s != me)
            def _():
                send[s] = got[j * cap:(j + 1) * cap]
                d_copy(s).start()
            @pl.when(s == me)
            def _():
                rows_in[0, me] = got[j * cap:(j + 1) * cap]
        return 0

    lax.fori_loop(1, nz + 1, dispatch, 0)

    def pass_on(p, _):
        far_piece(p).wait_recv()
        relay(p).start()
        return 0

    def share(z):
        for j in range(2):
            s = 2 * z + j
            @pl.when(s != me)
            def _():
                d_arrival(s).wait_recv()
            far_rows(s).start()
            near_rows(s).start()

    def pass_rows(z):
        for j in range(2):
            far_rows(2 * z + j).wait_recv()
            relay_rows(2 * z + j).start()

    def gated(z):
        for j in range(2):
            near_rows(2 * z + j).wait_recv()
        for j in range(2):
            relay_rows(2 * z + j).wait_recv()
        x = rows_in[:, pl.ds(2 * z, 2)].reshape(4 * 2 * cap, d_model)
        gate = jnp.dot(x, gu[:, :ff], preferred_element_type=jnp.float32)
        upper = jnp.dot(x, gu[:, ff:], preferred_element_type=jnp.float32)
        hidden = (gate / (1.0 + jnp.exp(-gate)) * upper).astype(jnp.bfloat16)
        hid_in[z, :, :ff] = hidden[:2 * cap]
        for k in range(1, 4):
            hid_out[z, k - 1] = hidden[2 * k * cap:2 * (k + 1) * cap]
        for k in (2, 3, 1):
            h_copy(z, k).start()

    def give_back(z):
        for k in range(1, 4):
            h_copy(z, k).wait_recv()
        down = jnp.dot(hid_in[z], dw[...], preferred_element_type=jnp.float32).astype(jnp.bfloat16)
        for j in range(2):
            s = 2 * z + j
            @pl.when(s != me)
            def _():
                ret[s] = down[j * cap:(j + 1) * cap]
                r_copy(s).start()
            @pl.when(s == me)
            def _():
                back[me] = down[j * cap:(j + 1) * cap]

    lax.fori_loop(0, PIECES // 2, pass_on, 0)
    share(0)
    pass_rows(0)
    own_loads[1].wait()
    own_loads[2].wait()
    gated(0)
    lax.fori_loop(PIECES // 2, PIECES, pass_on, 0)
    w_copy.wait_recv()

    def relayed(p, _):
        relay(p).wait_recv()
        return 0

    lax.fori_loop(0, PIECES, relayed, 0)

    def work(z, _):
        share(z)
        give_back(z - 1)
        pass_rows(z)
        gated(z)
        return 0

    lax.fori_loop(1, nz, work, 0)
    give_back(nz - 1)

    def arrive(s, _):
        @pl.when(s != me)
        def _():
            r_arrival(s).wait_recv()
        return 0

    lax.fori_loop(0, n, arrive, 0)
    for q in range(PARTS):
        cols = slice(q * span, (q + 1) * span)
        results = back[:, :, cols].reshape(n * cap, span)
        routed = jnp.dot(blend_hi[...], results, preferred_element_type=jnp.float32)
        routed = routed + jnp.dot(blend_lo[...], results, preferred_element_type=jnp.float32)
        out_ref[:, cols] = (stream_out[:, cols] + routed).astype(jnp.bfloat16)

    finish_attention()
    w_copy.wait_send()

    def passed(p, _):
        far_piece(p).wait_send()
        relay(p).wait_send()
        return 0

    lax.fori_loop(0, PIECES, passed, 0)

    def shared(z, _):
        for k in range(1, 4):
            h_copy(z, k).wait_send()
        return 0

    lax.fori_loop(0, nz, shared, 0)

    def finish(s, _):
        near_rows(s).wait_send()
        far_rows(s).wait_send()
        relay_rows(s).wait_send()
        @pl.when(s != me)
        def _():
            d_copy(s).wait_send()
            r_copy(s).wait_send()
        return 0

    lax.fori_loop(0, n, finish, 0)


def layer(n, nt, cap, *args):
    q1, ow, stream_in = args[0], args[7], args[8]
    rows = q1.shape[0]
    tokens, d = stream_in.shape
    vm = pl.BlockSpec(memory_space=pltpu.VMEM)
    hbm = pl.BlockSpec(memory_space=pl.ANY)
    sm = pl.BlockSpec(memory_space=pltpu.SMEM)
    chunk = rows // nt
    dma = pltpu.SemaphoreType.DMA
    bf, f32 = jnp.bfloat16, jnp.float32
    in_specs = [vm, vm, hbm, hbm, hbm, sm, vm, hbm, vm, vm]
    out_shape = (jax.ShapeDtypeStruct((tokens, d), f32), jax.ShapeDtypeStruct((tokens, d), bf))
    out_specs = (vm, vm)
    scratch = [
        pltpu.VMEM((n, rows, 2 * HEAD_DIM + VAL_DIM), bf),
        pltpu.VMEM((2, 2 * rows, HEAD_DIM), bf),
        pltpu.VMEM((2, 2 * rows, 128), f32),
        pltpu.VMEM((2, 2 * rows, 128), f32),
        pltpu.VMEM((2, 2 * rows, VAL_DIM), f32),
        pltpu.VMEM((rows, 2 * VAL_DIM), bf),
        pltpu.VMEM(ow.shape, bf),
        pltpu.VMEM((2 * chunk, d), bf),
        pltpu.VMEM((2 * chunk, d), bf),
        pltpu.VMEM((chunk, d), bf),
        pltpu.VMEM((chunk, d), bf),
        dma((4,)), dma((n // 2,)), dma((n // 2,)), dma((n // 2,)), dma((n // 2,)), dma((2, PARTS)), dma((2, PARTS)),
    ]
    if cap:
        ff = args[12].shape[2]
        in_specs = in_specs + [vm, vm, hbm, hbm, hbm]
        out_shape = jax.ShapeDtypeStruct((tokens, d), bf)
        out_specs = vm
        scratch = scratch + [
            pltpu.VMEM((tokens, d), f32),
            pltpu.VMEM((tokens, d), bf),
            pltpu.VMEM((d, 2 * ff), bf),
            pltpu.VMEM((nt * ff, d), bf),
            pltpu.VMEM((n * cap, tokens), bf),
            pltpu.VMEM((tokens, n * cap), bf),
            pltpu.VMEM((tokens, n * cap), bf),
            pltpu.VMEM((n, cap, d), bf),
            pltpu.VMEM((4, n, cap, d), bf),
            pltpu.VMEM((n // 2, 3, 2 * cap, ff), bf),
            pltpu.VMEM((n // 2, 2 * cap, 4 * ff), bf),
            pltpu.VMEM((n, cap, d), bf),
            pltpu.VMEM((n, cap, d), bf),
            dma((3,)), dma((1,)), dma((1,)),
        ] + [dma((PIECES,))] * 4 + [dma((n,))] * 2 + [dma((3, n))] * 2 + [dma((3, n // 2))] * 2 + [dma((n,))] * 2
    return pl.pallas_call(
        functools.partial(layer_kernel, n, nt, cap),
        out_shape=out_shape,
        in_specs=in_specs,
        out_specs=out_specs,
        scratch_shapes=scratch,
        compiler_params=pltpu.CompilerParams(
            collective_id=0, has_side_effects=True, vmem_limit_bytes=58 * 2**20
        ),
        name="layer",
    )(*args)


def shards(
    stream_in,
    queries_one,
    queries_two,
    keys_one,
    keys_two,
    values,
    lambdas,
    head_gain,
    out_weight,
    norm_gain,
    expert_ids,
    route_weight,
    gate_weight,
    up_weight,
    down_weight,
):
    n, nt = lax.axis_size("sp"), lax.axis_size("tp")
    rows_here = stream_in.shape[0]
    top_count = expert_ids.shape[1]
    slot_cap = 2 * top_count * rows_here // n
    shared = (
        queries_one, queries_two, keys_one, keys_two, values, lambdas,
        head_gain.reshape(1, -1), out_weight, stream_in, norm_gain.reshape(1, -1),
    )
    if slot_cap % 16 == 0:
        return layer(
            n, nt, slot_cap, *shared, expert_ids.T, route_weight.T, gate_weight, up_weight, down_weight
        )
    stream, normed = layer(n, nt, 0, *shared)
    flat_ids = expert_ids.reshape(-1)
    count = flat_ids.shape[0]
    order = lax.iota(jnp.int32, count)
    earlier = (flat_ids[None, :] == flat_ids[:, None]) & (order[None, :] < order[:, None])
    ranks = jnp.sum(earlier.astype(jnp.int32), axis=1)
    slots = flat_ids * slot_cap + ranks
    slot_of = slots.reshape(rows_here, top_count)
    places = lax.iota(jnp.int32, n * slot_cap)
    selector = sum(
        (slot_of[:, k][None, :] == places[:, None]).astype(jnp.bfloat16) for k in range(top_count)
    )
    send_rows = jnp.dot(selector, normed, preferred_element_type=jnp.float32).astype(jnp.bfloat16)
    received = lax.all_to_all(send_rows, "sp", split_axis=0, concat_axis=0, tiled=True)
    picked_rows = lax.all_gather(received, "tp", axis=0, tiled=True)
    gate = jnp.dot(picked_rows, gate_weight[0], preferred_element_type=jnp.float32)
    upper = jnp.dot(picked_rows, up_weight[0], preferred_element_type=jnp.float32)
    hidden = (jax.nn.silu(gate) * upper).astype(jnp.bfloat16)
    summed = lax.psum_scatter(
        jnp.dot(hidden, down_weight[0], preferred_element_type=jnp.float32).astype(jnp.bfloat16),
        "tp",
        scatter_dimension=0,
        tiled=True,
    )
    returned = lax.all_to_all(summed, "sp", split_axis=0, concat_axis=0, tiled=True)
    picked = jnp.take(returned, slots, axis=0).reshape(rows_here, top_count, -1).astype(jnp.float32)
    routed = jnp.sum(picked * route_weight[:, :, None], axis=1)
    return (stream + routed).astype(jnp.bfloat16)


def solution(mesh):
    return jax.shard_map(
        shards,
        mesh=mesh,
        in_specs=(
            P(("sp", "tp"), None),
            P("sp", "tp"),
            P("sp", "tp"),
            P("sp", "tp"),
            P("sp", "tp"),
            P("sp", "tp"),
            P("tp"),
            P(),
            P("tp", None),
            P(),
            P(("sp", "tp"), None),
            P(("sp", "tp"), None),
            P("sp", None, "tp"),
            P("sp", None, "tp"),
            P("sp", "tp", None),
        ),
        out_specs=P(("sp", "tp"), None),
        check_vma=False,
    )
```

```python
import functools

import jax
import jax.numpy as jnp
from jax import lax
from jax.experimental import pallas as pl
from jax.experimental.pallas import tpu as pltpu
from jax.sharding import PartitionSpec as P

HEAD_DIM = 128
VAL_DIM = 256


EPS = 1e-06
OUT_SCALE = 0.8


MESH = pl.DeviceIdType.MESH
LOG2E = 1.4426950408889634
PIECES = 8
HALVES = 2
PARTS = 4


def remote(src, dst, send_sem, recv_sem, where):
    return pltpu.make_async_remote_copy(
        src_ref=src,
        dst_ref=dst,
        send_sem=send_sem,
        recv_sem=recv_sem,
        device_id=where,
        device_id_type=MESH,
    )


def greet(devices, count):
    barrier = pltpu.get_barrier_semaphore()
    devices(lambda where: pl.semaphore_signal(barrier, inc=1, device_id=where, device_id_type=MESH))
    pl.semaphore_wait(barrier, count)


def layer_kernel(n, nt, cap, *refs):
    (
        q1_ref, q2_ref, k1_ref, k2_ref, v_ref, lam_ref, gain_ref, ow_ref, stream_ref, norm_ref,
    ) = refs[:10]
    if cap:
        ids_ref, route_ref, gw_ref, uw_ref, dw_ref, out_ref = refs[10:16]
        refs = refs[16:]
    else:
        stream_out, normed_out = refs[10:12]
        refs = refs[12:]
    kv, qs, top, total, acc, heads, ow, near_part, near_got, far_part, far_got = refs[:11]
    local_sem, z_send, z_recv, y_send, y_recv, p_send, p_recv = refs[11:18]
    if cap:
        (
            stream_out, normed_out, gu, dw, blend, blend_hi, blend_lo, send, rows_in, hid_out, hid_in, ret, back,
            own_sem, w_send, w_recv, f_send, f_recv, g_send, g_recv, d_send, d_recv,
            a_send, a_recv, h_send, h_recv, r_send, r_recv,
        ) = refs[18:]

    me, tp = lax.axis_index("sp"), lax.axis_index("tp")
    nz = n // 2
    zi, y = me // 2, lax.rem(me, 2)
    pair = me + 1 - 2 * y
    rows = q1_ref.shape[0]
    hd = HEAD_DIM
    chunk = rows // nt
    side, core = tp // 2, lax.rem(tp, 2)
    near = (me, tp + 1 - 2 * core)
    far = (me, lax.rem(tp + 2, 4))
    cross = (me, 3 - tp)

    loads = [
        pltpu.make_async_copy(k1_ref, kv.at[me, :, pl.ds(0, hd)], local_sem.at[0]),
        pltpu.make_async_copy(k2_ref, kv.at[me, :, pl.ds(hd, hd)], local_sem.at[1]),
        pltpu.make_async_copy(v_ref, kv.at[me, :, pl.ds(2 * hd, VAL_DIM)], local_sem.at[2]),
    ]
    for load in loads:
        load.start()
    if cap:
        ff = gw_ref.shape[2]

        deep = ff // PIECES
        own_loads = [
            pltpu.make_async_copy(dw_ref.at[0], dw.at[pl.ds(0, ff), :], own_sem.at[0]),
            pltpu.make_async_copy(gw_ref.at[0], gu.at[:, pl.ds(0, ff)], own_sem.at[1]),
            pltpu.make_async_copy(uw_ref.at[0], gu.at[:, pl.ds(ff, ff)], own_sem.at[2]),
        ]
        for load in own_loads:
            load.start()
        w_copy = remote(dw.at[pl.ds(0, ff), :], dw.at[pl.ds(ff, ff), :], w_send.at[0], w_recv.at[0], near)

        def piece(p, k):
            return dw.at[pl.ds(pl.multiple_of(k * ff + p * deep, deep), deep), :]

        def far_piece(p):
            return remote(piece(p, 0), piece(p, 2), f_send.at[p], f_recv.at[p], far)

        def relay(p):
            return remote(piece(p, 2), piece(p, 3), g_send.at[p], g_recv.at[p], near)

        ahead = jnp.minimum(3 + 3 * zi, PIECES)

        def far_some(p, _):
            far_piece(p).start()
            return 0

    ow_load = pltpu.make_async_copy(ow_ref, ow, local_sem.at[3])
    ow_load.start()

    def peers(tell):
        def column(s, _):
            @pl.when(s != me)
            def _():
                tell((s, tp))
            return 0
        lax.fori_loop(0, n, column, 0)
        tell(near)
        tell(far)
        tell(cross)

    greet(peers, n - 1 + 3)
    for load in loads:
        load.wait()

    part_rows = rows // HALVES

    def block(b, c):
        return kv.at[b, pl.ds(c * part_rows, part_rows), :]

    def hop(z, c):
        b, i = 2 * z + y, HALVES * z + c
        return remote(block(b, c), block(b, c), z_send.at[i], z_recv.at[i], (lax.rem(me + 2, n), tp))

    def y_copy(z, c):
        b, i = 2 * z + y, HALVES * z + c
        return remote(block(b, c), block(b, c), y_send.at[i], y_recv.at[i], (pair, tp))

    def y_arrival(z, c):
        b, i = 2 * z + 1 - y, HALVES * z + c
        return remote(block(b, c), block(b, c), y_send.at[i], y_recv.at[i], (pair, tp))

    for c in range(HALVES):
        @pl.when(zi < nz - 1)
        def _():
            hop(zi, c).start()

        @pl.when(y == 0)
        def _():
            y_copy(zi, c).start()

    if cap:
        own_loads[0].wait()
        lax.fori_loop(0, ahead, far_some, 0)
        w_copy.start()

    for i, ref in enumerate((q1_ref, q2_ref)):
        for h in range(2):
            qs[i, h * rows:(h + 1) * rows, :] = ref[:, h * hd:(h + 1) * hd]

    scale = HEAD_DIM ** (-0.5) * LOG2E

    def fold(b, first):
        vals = kv[b, :, 2 * hd:]
        for i in range(2):
            keys = kv[b, :, i * hd:(i + 1) * hd]
            s = lax.dot_general(qs[i], keys, (((1,), (1,)), ((), ())), preferred_element_type=jnp.float32)
            if first:
                r = lax.broadcasted_iota(jnp.int32, (2, rows, rows), 1).reshape(2 * rows, rows)
                c = lax.broadcasted_iota(jnp.int32, (2 * rows, rows), 1)
                s = jnp.where(c <= r, s, -jnp.inf)
                new = jnp.max(s, axis=-1, keepdims=True)
            else:
                old = top[i][:, :1]
                new = jnp.maximum(old, jnp.max(s, axis=-1, keepdims=True))
            e = jnp.exp2((s - new) * scale)
            part = sum(e[:, c * 128:(c + 1) * 128] for c in range(rows // 128))
            pv = jnp.dot(e.astype(jnp.bfloat16), vals, preferred_element_type=jnp.float32)
            if first:
                acc[i] = pv
                total[i] = part
            else:
                alpha = jnp.exp2((old - new) * scale)
                acc[i] = acc[i] * alpha + pv
                total[i] = total[i] * alpha + part
            top[i] = jnp.broadcast_to(new, (2 * rows, 128))

    fold(me, True)

    if cap:
        choices, tokens = ids_ref.shape
        which = lax.broadcasted_iota(jnp.int32, (max(n, 8), tokens), 0)
        named = [(ids_ref[k:k + 1, :] == which).astype(jnp.float32) for k in range(choices)]
        before = lax.broadcasted_iota(jnp.int32, (tokens, tokens), 0) < lax.broadcasted_iota(
            jnp.int32, (tokens, tokens), 1
        )
        counts = jnp.dot(
            sum(named).astype(jnp.bfloat16), before.astype(jnp.bfloat16), preferred_element_type=jnp.float32
        )
        place = lax.broadcasted_iota(jnp.int32, (n * cap, tokens), 0)
        chosen = jnp.zeros((n * cap, tokens), jnp.float32)
        weight = jnp.zeros((n * cap, tokens), jnp.float32)
        for k in range(choices):
            rank = jnp.sum(named[k] * counts, axis=0, keepdims=True).astype(jnp.int32)
            hit = (ids_ref[k:k + 1, :] * cap + rank) == place
            chosen = chosen + hit.astype(jnp.float32)
            weight = weight + jnp.where(hit, route_ref[k:k + 1, :], 0.0)
        blend[...] = chosen.astype(jnp.bfloat16)
        weight = weight.T
        coarse = weight.astype(jnp.bfloat16)
        blend_hi[...] = coarse
        blend_lo[...] = (weight - coarse.astype(jnp.float32)).astype(jnp.bfloat16)

    def walk(d, _):
        z = zi - d
        @pl.when(d <= zi)
        def _():
            for c in range(HALVES):
                hop(z, c).wait_recv()
                y_copy(z, c).start()
                @pl.when(zi < nz - 1)
                def _():
                    hop(z, c).start()
            fold(2 * z + y, False)
        @pl.when(jnp.logical_or(d > 1, y == 1))
        def _():
            for c in range(HALVES):
                y_arrival(z + 1, c).wait_recv()
            fold(2 * (z + 1) + 1 - y, False)
        return 0

    lax.fori_loop(1, jnp.where(zi + y > 0, zi + 2, 1), walk, 0)

    for h in range(2):
        r = pl.ds(h * rows, rows)
        one = acc[0, r, :] / jnp.sum(total[0, r, :], axis=-1, keepdims=True)
        two = acc[1, r, :] / jnp.sum(total[1, r, :], axis=-1, keepdims=True)
        diff = one - lam_ref[h] * two
        ms = jnp.mean(diff * diff, axis=-1, keepdims=True)
        heads[:, h * VAL_DIM:(h + 1) * VAL_DIM] = (
            diff * lax.rsqrt(ms + EPS) * gain_ref[...] * OUT_SCALE
        ).astype(jnp.bfloat16)

    ow_load.wait()

    d_model = ow.shape[1]
    span = d_model // PARTS

    def picked(first, second):
        return jnp.concatenate(
            [heads[pl.ds(pl.multiple_of(t * chunk, chunk), chunk), :] for t in (first, second)], axis=0
        )

    def near_copy(q):
        cols = pl.ds(q * span, span)
        return remote(near_part.at[:, cols], near_got.at[:, cols], p_send.at[0, q], p_recv.at[0, q], near)

    def far_copy(q):
        cols = pl.ds(q * span, span)
        return remote(far_part.at[:, cols], far_got.at[:, cols], p_send.at[1, q], p_recv.at[1, q], far)

    away = 1 - side
    other = picked(2 * away + 1 - core, 2 * side + 1 - core)
    for q in range(PARTS):
        cols = slice(q * span, (q + 1) * span)
        near_part[:, cols] = jnp.dot(
            other, ow[:, cols], preferred_element_type=jnp.float32
        ).astype(jnp.bfloat16)
        near_copy(q).start()
    own = picked(2 * away + core, 2 * side + core)
    for q in range(PARTS):
        cols = slice(q * span, (q + 1) * span)
        mine = jnp.dot(own, ow[:, cols], preferred_element_type=jnp.float32)
        near_copy(q).wait_recv()
        mine = mine + near_got[:, cols].astype(jnp.float32)
        far_part[:, cols] = mine[:chunk].astype(jnp.bfloat16)
        far_copy(q).start()
        stream_out[:, cols] = stream_ref[:, cols].astype(jnp.float32) + mine[chunk:]
    if cap:
        lax.fori_loop(ahead, PIECES, far_some, 0)
    square = jnp.zeros((chunk, 1), jnp.float32)
    for q in range(PARTS):
        cols = slice(q * span, (q + 1) * span)
        far_copy(q).wait_recv()
        summed = stream_out[:, cols] + far_got[:, cols].astype(jnp.float32)
        stream_out[:, cols] = summed
        square = square + jnp.sum(summed * summed, axis=-1, keepdims=True)
    normed_out[...] = (
        stream_out[...] * lax.rsqrt(square * (1.0 / d_model) + EPS) * norm_ref[...]
    ).astype(jnp.bfloat16)

    def finish_attention():
        for q in range(PARTS):
            near_copy(q).wait_send()
            far_copy(q).wait_send()

        for c in range(HALVES):
            @pl.when(y == 0)
            def _():
                y_copy(zi, c).wait_send()

            @pl.when(zi < nz - 1)
            def _():
                hop(zi, c).wait_send()

        def sent(z, _):
            for c in range(HALVES):
                y_copy(z, c).wait_send()
                @pl.when(zi < nz - 1)
                def _():
                    hop(z, c).wait_send()
            return 0

        lax.fori_loop(0, zi, sent, 0)

    if not cap:
        finish_attention()
        return

    def d_copy(s):
        return remote(send.at[s], rows_in.at[0, me], d_send.at[s], d_recv.at[me], (s, tp))

    def d_arrival(s):
        return remote(send.at[s], rows_in.at[0, s], d_send.at[s], d_recv.at[s], (s, tp))

    def near_rows(s):
        return remote(rows_in.at[0, s], rows_in.at[1, s], a_send.at[0, s], a_recv.at[0, s], near)

    def far_rows(s):
        return remote(rows_in.at[0, s], rows_in.at[2, s], a_send.at[1, s], a_recv.at[1, s], far)

    def relay_rows(s):
        return remote(rows_in.at[2, s], rows_in.at[3, s], a_send.at[2, s], a_recv.at[2, s], near)

    def h_copy(z, k):
        return remote(
            hid_out.at[z, k - 1],
            hid_in.at[z, :, pl.ds(k * ff, ff)],
            h_send.at[k - 1, z],
            h_recv.at[k - 1, z],
            (near, far, cross)[k - 1],
        )

    def r_copy(s):
        return remote(ret.at[s], back.at[me], r_send.at[s], r_recv.at[me], (s, tp))

    def r_arrival(s):
        return remote(ret.at[s], back.at[s], r_send.at[s], r_recv.at[s], (s, tp))

    def dispatch(d, _):
        z = jnp.where(zi >= nz // 2, d, nz - 1 - d)
        base = pl.multiple_of(2 * z * cap, 2 * cap)
        got = jnp.dot(
            blend[pl.ds(base, 2 * cap), :], normed_out[...], preferred_element_type=jnp.float32
        ).astype(jnp.bfloat16)
        for j in range(2):
            s = 2 * z + j
            @pl.when(s != me)
            def _():
                send[s] = got[j * cap:(j + 1) * cap]
                d_copy(s).start()
            @pl.when(s == me)
            def _():
                rows_in[0, me] = got[j * cap:(j + 1) * cap]
        return 0

    lax.fori_loop(0, nz, dispatch, 0)

    def pass_on(p, _):
        far_piece(p).wait_recv()
        relay(p).start()
        return 0

    def share(z):
        for j in range(2):
            s = 2 * z + j
            @pl.when(s != me)
            def _():
                d_arrival(s).wait_recv()
            far_rows(s).start()
            near_rows(s).start()

    def pass_rows(z):
        for j in range(2):
            far_rows(2 * z + j).wait_recv()
            relay_rows(2 * z + j).start()

    def gated(z):
        for j in range(2):
            near_rows(2 * z + j).wait_recv()
        for j in range(2):
            relay_rows(2 * z + j).wait_recv()
        x = rows_in[:, pl.ds(2 * z, 2)].reshape(4 * 2 * cap, d_model)
        gate = jnp.dot(x, gu[:, :ff], preferred_element_type=jnp.float32)
        upper = jnp.dot(x, gu[:, ff:], preferred_element_type=jnp.float32)
        hidden = (gate / (1.0 + jnp.exp(-gate)) * upper).astype(jnp.bfloat16)
        hid_in[z, :, :ff] = hidden[:2 * cap]
        for k in range(1, 4):
            hid_out[z, k - 1] = hidden[2 * k * cap:2 * (k + 1) * cap]
        for k in (2, 3, 1):
            h_copy(z, k).start()

    def give_back(z):
        for k in range(1, 4):
            h_copy(z, k).wait_recv()
        down = jnp.dot(hid_in[z], dw[...], preferred_element_type=jnp.float32).astype(jnp.bfloat16)
        for j in range(2):
            s = 2 * z + j
            @pl.when(s != me)
            def _():
                ret[s] = down[j * cap:(j + 1) * cap]
                r_copy(s).start()
            @pl.when(s == me)
            def _():
                back[me] = down[j * cap:(j + 1) * cap]

    early = zi >= nz // 2
    share(0)
    @pl.when(early)
    def _():
        share(1)
    lax.fori_loop(0, PIECES, pass_on, 0)
    own_loads[1].wait()
    own_loads[2].wait()
    w_copy.wait_recv()

    def relayed(p, _):
        relay(p).wait_recv()
        return 0

    lax.fori_loop(0, PIECES, relayed, 0)

    def work(z, _):
        pass_rows(z)
        gated(z)
        ahead_z = jnp.where(early, z + 2, z + 1)
        @pl.when(ahead_z < nz)
        def _():
            share(ahead_z)
        behind_z = jnp.where(early, z - 1, z)
        @pl.when(behind_z >= 0)
        def _():
            give_back(behind_z)
        return 0

    lax.fori_loop(0, nz, work, 0)
    @pl.when(early)
    def _():
        give_back(nz - 1)

    def arrive(s, _):
        @pl.when(s != me)
        def _():
            r_arrival(s).wait_recv()
        return 0

    lax.fori_loop(0, n, arrive, 0)
    for q in range(PARTS):
        cols = slice(q * span, (q + 1) * span)
        results = back[:, :, cols].reshape(n * cap, span)
        routed = jnp.dot(blend_hi[...], results, preferred_element_type=jnp.float32)
        routed = routed + jnp.dot(blend_lo[...], results, preferred_element_type=jnp.float32)
        out_ref[:, cols] = (stream_out[:, cols] + routed).astype(jnp.bfloat16)

    finish_attention()
    w_copy.wait_send()

    def passed(p, _):
        far_piece(p).wait_send()
        relay(p).wait_send()
        return 0

    lax.fori_loop(0, PIECES, passed, 0)

    def shared(z, _):
        for k in range(1, 4):
            h_copy(z, k).wait_send()
        return 0

    lax.fori_loop(0, nz, shared, 0)

    def finish(s, _):
        near_rows(s).wait_send()
        far_rows(s).wait_send()
        relay_rows(s).wait_send()
        @pl.when(s != me)
        def _():
            d_copy(s).wait_send()
            r_copy(s).wait_send()
        return 0

    lax.fori_loop(0, n, finish, 0)


def layer(n, nt, cap, *args):
    q1, ow, stream_in = args[0], args[7], args[8]
    rows = q1.shape[0]
    tokens, d = stream_in.shape
    vm = pl.BlockSpec(memory_space=pltpu.VMEM)
    hbm = pl.BlockSpec(memory_space=pl.ANY)
    sm = pl.BlockSpec(memory_space=pltpu.SMEM)
    chunk = rows // nt
    dma = pltpu.SemaphoreType.DMA
    bf, f32 = jnp.bfloat16, jnp.float32
    in_specs = [vm, vm, hbm, hbm, hbm, sm, vm, hbm, vm, vm]
    out_shape = (jax.ShapeDtypeStruct((tokens, d), f32), jax.ShapeDtypeStruct((tokens, d), bf))
    out_specs = (vm, vm)
    scratch = [
        pltpu.VMEM((n, rows, 2 * HEAD_DIM + VAL_DIM), bf),
        pltpu.VMEM((2, 2 * rows, HEAD_DIM), bf),
        pltpu.VMEM((2, 2 * rows, 128), f32),
        pltpu.VMEM((2, 2 * rows, 128), f32),
        pltpu.VMEM((2, 2 * rows, VAL_DIM), f32),
        pltpu.VMEM((rows, 2 * VAL_DIM), bf),
        pltpu.VMEM(ow.shape, bf),
        pltpu.VMEM((2 * chunk, d), bf),
        pltpu.VMEM((2 * chunk, d), bf),
        pltpu.VMEM((chunk, d), bf),
        pltpu.VMEM((chunk, d), bf),
        dma((4,)), dma((n // 2 * HALVES,)), dma((n // 2 * HALVES,)), dma((n // 2 * HALVES,)), dma((n // 2 * HALVES,)), dma((2, PARTS)), dma((2, PARTS)),
    ]
    if cap:
        ff = args[12].shape[2]
        in_specs = in_specs + [vm, vm, hbm, hbm, hbm]
        out_shape = jax.ShapeDtypeStruct((tokens, d), bf)
        out_specs = vm
        scratch = scratch + [
            pltpu.VMEM((tokens, d), f32),
            pltpu.VMEM((tokens, d), bf),
            pltpu.VMEM((d, 2 * ff), bf),
            pltpu.VMEM((nt * ff, d), bf),
            pltpu.VMEM((n * cap, tokens), bf),
            pltpu.VMEM((tokens, n * cap), bf),
            pltpu.VMEM((tokens, n * cap), bf),
            pltpu.VMEM((n, cap, d), bf),
            pltpu.VMEM((4, n, cap, d), bf),
            pltpu.VMEM((n // 2, 3, 2 * cap, ff), bf),
            pltpu.VMEM((n // 2, 2 * cap, 4 * ff), bf),
            pltpu.VMEM((n, cap, d), bf),
            pltpu.VMEM((n, cap, d), bf),
            dma((3,)), dma((1,)), dma((1,)),
        ] + [dma((PIECES,))] * 4 + [dma((n,))] * 2 + [dma((3, n))] * 2 + [dma((3, n // 2))] * 2 + [dma((n,))] * 2
    return pl.pallas_call(
        functools.partial(layer_kernel, n, nt, cap),
        out_shape=out_shape,
        in_specs=in_specs,
        out_specs=out_specs,
        scratch_shapes=scratch,
        compiler_params=pltpu.CompilerParams(
            collective_id=0, has_side_effects=True, vmem_limit_bytes=58 * 2**20
        ),
        name="layer",
    )(*args)


def shards(
    stream_in,
    queries_one,
    queries_two,
    keys_one,
    keys_two,
    values,
    lambdas,
    head_gain,
    out_weight,
    norm_gain,
    expert_ids,
    route_weight,
    gate_weight,
    up_weight,
    down_weight,
):
    n, nt = lax.axis_size("sp"), lax.axis_size("tp")
    rows_here = stream_in.shape[0]
    top_count = expert_ids.shape[1]
    slot_cap = 2 * top_count * rows_here // n
    shared = (
        queries_one, queries_two, keys_one, keys_two, values, lambdas,
        head_gain.reshape(1, -1), out_weight, stream_in, norm_gain.reshape(1, -1),
    )
    if slot_cap % 16 == 0:
        return layer(
            n, nt, slot_cap, *shared, expert_ids.T, route_weight.T, gate_weight, up_weight, down_weight
        )
    stream, normed = layer(n, nt, 0, *shared)
    flat_ids = expert_ids.reshape(-1)
    count = flat_ids.shape[0]
    order = lax.iota(jnp.int32, count)
    earlier = (flat_ids[None, :] == flat_ids[:, None]) & (order[None, :] < order[:, None])
    ranks = jnp.sum(earlier.astype(jnp.int32), axis=1)
    slots = flat_ids * slot_cap + ranks
    slot_of = slots.reshape(rows_here, top_count)
    places = lax.iota(jnp.int32, n * slot_cap)
    selector = sum(
        (slot_of[:, k][None, :] == places[:, None]).astype(jnp.bfloat16) for k in range(top_count)
    )
    send_rows = jnp.dot(selector, normed, preferred_element_type=jnp.float32).astype(jnp.bfloat16)
    received = lax.all_to_all(send_rows, "sp", split_axis=0, concat_axis=0, tiled=True)
    picked_rows = lax.all_gather(received, "tp", axis=0, tiled=True)
    gate = jnp.dot(picked_rows, gate_weight[0], preferred_element_type=jnp.float32)
    upper = jnp.dot(picked_rows, up_weight[0], preferred_element_type=jnp.float32)
    hidden = (jax.nn.silu(gate) * upper).astype(jnp.bfloat16)
    summed = lax.psum_scatter(
        jnp.dot(hidden, down_weight[0], preferred_element_type=jnp.float32).astype(jnp.bfloat16),
        "tp",
        scatter_dimension=0,
        tiled=True,
    )
    returned = lax.all_to_all(summed, "sp", split_axis=0, concat_axis=0, tiled=True)
    picked = jnp.take(returned, slots, axis=0).reshape(rows_here, top_count, -1).astype(jnp.float32)
    routed = jnp.sum(picked * route_weight[:, :, None], axis=1)
    return (stream + routed).astype(jnp.bfloat16)


def solution(mesh):
    return jax.shard_map(
        shards,
        mesh=mesh,
        in_specs=(
            P(("sp", "tp"), None),
            P("sp", "tp"),
            P("sp", "tp"),
            P("sp", "tp"),
            P("sp", "tp"),
            P("sp", "tp"),
            P("tp"),
            P(),
            P("tp", None),
            P(),
            P(("sp", "tp"), None),
            P(("sp", "tp"), None),
            P("sp", None, "tp"),
            P("sp", None, "tp"),
            P("sp", "tp", None),
        ),
        out_specs=P(("sp", "tp"), None),
        check_vma=False,
    )
```

```python
import functools

import jax
import jax.numpy as jnp
from jax import lax
from jax.experimental import pallas as pl
from jax.experimental.pallas import tpu as pltpu
from jax.sharding import PartitionSpec as P

HEAD_DIM = 128
VAL_DIM = 256


EPS = 1e-06
OUT_SCALE = 0.8


MESH = pl.DeviceIdType.MESH
LOG2E = 1.4426950408889634
DEEP = 8
WIDE = 8
DOWN = ((0, 2), (2, 2), (4, 2), (6, 1), (7, 1))
PARTS = 4
HALVES = 2


def remote(src, dst, send_sem, recv_sem, where):
    return pltpu.make_async_remote_copy(
        src_ref=src,
        dst_ref=dst,
        send_sem=send_sem,
        recv_sem=recv_sem,
        device_id=where,
        device_id_type=MESH,
    )


def greet(devices, count):
    barrier = pltpu.get_barrier_semaphore()
    devices(lambda where: pl.semaphore_signal(barrier, inc=1, device_id=where, device_id_type=MESH))
    pl.semaphore_wait(barrier, count)


def layer_kernel(n, nt, cap, *refs):
    (
        q1_ref, q2_ref, k1_ref, k2_ref, v_ref, lam_ref, gain_ref, ow_ref, stream_ref, norm_ref,
    ) = refs[:10]
    if cap:
        ids_ref, route_ref, gw_ref, uw_ref, dw_ref, out_ref = refs[10:16]
        refs = refs[16:]
    else:
        stream_out, normed_out = refs[10:12]
        refs = refs[12:]
    kv, qs, top, total, acc, heads, ow, stream, near_part, near_got, far_part, far_got = refs[:12]
    local_sem, z_send, z_recv, y_send, y_recv, p_send, p_recv = refs[12:19]
    if cap:
        (
            stream_out, normed_out, gu, dw, blend, blend_hi, blend_lo, send, rows_in, hid, ret, back,
            chain, own_sem, w_send, w_recv, f_send, f_recv, g_send, g_recv, d_send, d_recv, r_send, r_recv,
        ) = refs[19:]

    me, tp = lax.axis_index("sp"), lax.axis_index("tp")
    nz = n // 2
    zi, y = me // 2, lax.rem(me, 2)
    pair = me + 1 - 2 * y
    rows = q1_ref.shape[0]
    hd = HEAD_DIM
    chunk = rows // nt
    side, core = tp // 2, lax.rem(tp, 2)
    near = (me, tp + 1 - 2 * core)
    far = (me, lax.rem(tp + 2, 4))

    loads = [
        pltpu.make_async_copy(k1_ref, kv.at[me, :, pl.ds(0, hd)], local_sem.at[0]),
        pltpu.make_async_copy(k2_ref, kv.at[me, :, pl.ds(hd, hd)], local_sem.at[1]),
        pltpu.make_async_copy(v_ref, kv.at[me, :, pl.ds(2 * hd, VAL_DIM)], local_sem.at[2]),
    ]
    rest = [
        pltpu.make_async_copy(
            ref.at[:, pl.ds(h * hd, hd)], qs.at[i, pl.ds(h * rows, rows), :], local_sem.at[4 + 2 * i + h]
        )
        for i, ref in enumerate((q1_ref, q2_ref))
        for h in range(2)
    ]
    stream_load = pltpu.make_async_copy(stream_ref, stream, local_sem.at[8])
    for load in loads + rest:
        load.start()
    stream_load.start()
    if cap:
        ff = gw_ref.shape[2]

        deep = gu.shape[1] // DEEP
        wide = dw.shape[1] // WIDE

        def part_of(i, k):
            if i == 2:
                return dw.at[pl.ds(k * ff, ff), :]
            return gu.at[i, :, pl.ds(k * ff, ff)]

        own_loads = [
            pltpu.make_async_copy(ref.at[0], part_of(i, 0), own_sem.at[i])
            for i, ref in enumerate((gw_ref, uw_ref, dw_ref))
        ]
        for load in own_loads:
            load.start()

        def w_copy(i):
            return remote(part_of(i, 0), part_of(i, 1), w_send.at[i], w_recv.at[i], near)

        def piece(p, k):
            rows_of = pl.ds(pl.multiple_of(lax.rem(p, DEEP) * deep, deep), deep)
            return gu.at[p // DEEP, rows_of, pl.ds(k * ff, ff)]

        def far_piece(p):
            return remote(piece(p, 0), piece(p, 2), f_send.at[p], f_recv.at[p], far)

        def relay(p):
            return remote(piece(p, 2), piece(p, 3), g_send.at[p], g_recv.at[p], near)

        def down_piece(j, k):
            first, count = DOWN[j]
            return dw.at[pl.ds(k * ff, ff), pl.ds(first * wide, count * wide)]

        def far_down(j):
            p = 2 * DEEP + j
            return remote(down_piece(j, 0), down_piece(j, 2), f_send.at[p], f_recv.at[p], far)

        def relay_down(j):
            p = 2 * DEEP + j
            return remote(down_piece(j, 2), down_piece(j, 3), g_send.at[p], g_recv.at[p], near)

        ahead = jnp.minimum(jnp.where(zi == 0, 3 + y, jnp.where(zi == nz - 1, 9, 4 + 2 * zi)), 2 * DEEP)

        def far_some(p, _):
            far_piece(p).start()
            return 0

    ow_load = pltpu.make_async_copy(ow_ref, ow, local_sem.at[3])
    ow_load.start()

    below, above = zi > 0, zi < nz - 1

    def peers(tell):
        tell(near)
        tell(far)
        tell((pair, tp))
        @pl.when(below)
        def _():
            tell((me - 2, tp))
        @pl.when(above)
        def _():
            tell((me + 2, tp))

    greet(peers, 3 + below.astype(jnp.int32) + above.astype(jnp.int32))
    for load in loads:
        load.wait()

    part_rows = rows // HALVES

    def block(b, c):
        return kv.at[b, pl.ds(c * part_rows, part_rows), :]

    def hop(z, c):
        b, i = 2 * z + y, HALVES * z + c
        return remote(block(b, c), block(b, c), z_send.at[i], z_recv.at[i], (jnp.minimum(me + 2, n - 2 + y), tp))

    def y_copy(z, c):
        b, i = 2 * z + y, HALVES * z + c
        return remote(block(b, c), block(b, c), y_send.at[i], y_recv.at[i], (pair, tp))

    def y_arrival(z, c):
        b, i = 2 * z + 1 - y, HALVES * z + c
        return remote(block(b, c), block(b, c), y_send.at[i], y_recv.at[i], (pair, tp))

    for c in range(HALVES):
        @pl.when(zi < nz - 1)
        def _():
            hop(zi, c).start()

        @pl.when(y == 0)
        def _():
            y_copy(zi, c).start()

    if cap:
        own_loads[0].wait()
        own_loads[1].wait()
        lax.fori_loop(0, ahead, far_some, 0)
        own_loads[2].wait()
        for i in range(3):
            w_copy(i).start()

    for load in rest:
        load.wait()

    scale = HEAD_DIM ** (-0.5) * LOG2E

    def fold(b, first):
        vals = kv[b, :, 2 * hd:]
        for i in range(2):
            keys = kv[b, :, i * hd:(i + 1) * hd]
            s = lax.dot_general(qs[i], keys, (((1,), (1,)), ((), ())), preferred_element_type=jnp.float32)
            if first:
                r = lax.broadcasted_iota(jnp.int32, (2, rows, rows), 1).reshape(2 * rows, rows)
                c = lax.broadcasted_iota(jnp.int32, (2 * rows, rows), 1)
                s = jnp.where(c <= r, s, -jnp.inf)
            new = jnp.broadcast_to(jnp.max(s, axis=-1, keepdims=True), (2 * rows, 128))
            if not first:
                old = top[i]
                new = jnp.maximum(old, new)
            terms = [jnp.exp2((s[:, c:c + 128] - new) * scale) for c in range(0, rows, 128)]
            weights = jnp.concatenate([e.astype(jnp.bfloat16) for e in terms], axis=1)
            pv = jnp.dot(weights, vals, preferred_element_type=jnp.float32)
            if first:
                acc[i] = pv
                total[i] = sum(terms)
            else:
                alpha = jnp.exp2((old - new) * scale)
                for c in range(0, VAL_DIM, 128):
                    acc[i, :, c:c + 128] = acc[i, :, c:c + 128] * alpha + pv[:, c:c + 128]
                total[i] = total[i] * alpha + sum(terms)
            top[i] = new

    fold(me, True)

    if cap:
        for side_sem, source, target, where in ((0, above, below, me - 2), (1, below, above, me + 2)):
            @pl.when(source)
            def _():
                pl.semaphore_wait(chain.at[side_sem], 1)
            @pl.when(target)
            def _():
                pl.semaphore_signal(chain.at[side_sem], inc=1, device_id=(where, tp), device_id_type=MESH)

    if cap:
        choices, tokens = ids_ref.shape
        which = lax.broadcasted_iota(jnp.int32, (max(n, 8), tokens), 0)
        named = [(ids_ref[k:k + 1, :] == which).astype(jnp.float32) for k in range(choices)]
        before = lax.broadcasted_iota(jnp.int32, (tokens, tokens), 0) < lax.broadcasted_iota(
            jnp.int32, (tokens, tokens), 1
        )
        counts = jnp.dot(
            sum(named).astype(jnp.bfloat16), before.astype(jnp.bfloat16), preferred_element_type=jnp.float32
        )
        place = lax.broadcasted_iota(jnp.int32, (n * cap, tokens), 0)
        chosen = jnp.zeros((n * cap, tokens), jnp.float32)
        weight = jnp.zeros((n * cap, tokens), jnp.float32)
        for k in range(choices):
            rank = jnp.sum(named[k] * counts, axis=0, keepdims=True).astype(jnp.int32)
            hit = (ids_ref[k:k + 1, :] * cap + rank) == place
            chosen = chosen + hit.astype(jnp.float32)
            weight = weight + jnp.where(hit, route_ref[k:k + 1, :], 0.0)
        blend[...] = chosen.astype(jnp.bfloat16)
        weight = weight.T
        coarse = weight.astype(jnp.bfloat16)
        blend_hi[...] = coarse
        blend_lo[...] = (weight - coarse.astype(jnp.float32)).astype(jnp.bfloat16)

    def walk(d, _):
        z = zi - d
        @pl.when(d <= zi)
        def _():
            for c in range(HALVES):
                hop(z, c).wait_recv()
                y_copy(z, c).start()
                @pl.when(zi < nz - 1)
                def _():
                    hop(z, c).start()
            fold(2 * z + y, False)
        @pl.when(jnp.logical_or(d > 1, y == 1))
        def _():
            for c in range(HALVES):
                y_arrival(z + 1, c).wait_recv()
            fold(2 * (z + 1) + 1 - y, False)
        return 0

    lax.fori_loop(1, jnp.where(zi + y > 0, zi + 2, 1), walk, 0)

    for h in range(2):
        r = pl.ds(h * rows, rows)
        one = acc[0, r, :] / jnp.sum(total[0, r, :], axis=-1, keepdims=True)
        two = acc[1, r, :] / jnp.sum(total[1, r, :], axis=-1, keepdims=True)
        diff = one - lam_ref[h] * two
        ms = jnp.mean(diff * diff, axis=-1, keepdims=True)
        heads[:, h * VAL_DIM:(h + 1) * VAL_DIM] = (
            diff * lax.rsqrt(ms + EPS) * gain_ref[...] * OUT_SCALE
        ).astype(jnp.bfloat16)

    ow_load.wait()

    d_model = ow.shape[1]
    span = d_model // PARTS

    def picked(first, second):
        return jnp.concatenate(
            [heads[pl.ds(pl.multiple_of(t * chunk, chunk), chunk), :] for t in (first, second)], axis=0
        )

    def near_copy(q):
        cols = pl.ds(q * span, span)
        return remote(near_part.at[:, cols], near_got.at[:, cols], p_send.at[0, q], p_recv.at[0, q], near)

    def far_copy(q):
        cols = pl.ds(q * span, span)
        return remote(far_part.at[:, cols], far_got.at[:, cols], p_send.at[1, q], p_recv.at[1, q], far)

    away = 1 - side
    other = picked(2 * away + 1 - core, 2 * side + 1 - core)
    for q in range(PARTS):
        cols = slice(q * span, (q + 1) * span)
        near_part[:, cols] = jnp.dot(
            other, ow[:, cols], preferred_element_type=jnp.float32
        ).astype(jnp.bfloat16)
        near_copy(q).start()
    stream_load.wait()
    own = picked(2 * away + core, 2 * side + core)
    for q in range(PARTS):
        cols = slice(q * span, (q + 1) * span)
        mine = jnp.dot(own, ow[:, cols], preferred_element_type=jnp.float32)
        near_copy(q).wait_recv()
        mine = mine + near_got[:, cols].astype(jnp.float32)
        far_part[:, cols] = mine[:chunk].astype(jnp.bfloat16)
        far_copy(q).start()
        stream_out[:, cols] = stream[:, cols].astype(jnp.float32) + mine[chunk:]
    if cap:
        lax.fori_loop(ahead, 2 * DEEP, far_some, 0)
        for j in range(len(DOWN)):
            far_down(j).start()
    square = jnp.zeros((chunk, 1), jnp.float32)
    for q in range(PARTS):
        cols = slice(q * span, (q + 1) * span)
        far_copy(q).wait_recv()
        summed = stream_out[:, cols] + far_got[:, cols].astype(jnp.float32)
        stream_out[:, cols] = summed
        square = square + jnp.sum(summed * summed, axis=-1, keepdims=True)
    normed_out[...] = (
        stream_out[...] * lax.rsqrt(square * (1.0 / d_model) + EPS) * norm_ref[...]
    ).astype(jnp.bfloat16)

    def finish_attention():
        for q in range(PARTS):
            near_copy(q).wait_send()
            far_copy(q).wait_send()

        for c in range(HALVES):
            @pl.when(y == 0)
            def _():
                y_copy(zi, c).wait_send()

            @pl.when(zi < nz - 1)
            def _():
                hop(zi, c).wait_send()

        def sent(z, _):
            for c in range(HALVES):
                y_copy(z, c).wait_send()
                @pl.when(zi < nz - 1)
                def _():
                    hop(z, c).wait_send()
            return 0

        lax.fori_loop(0, zi, sent, 0)

    if not cap:
        finish_attention()
        return

    def d_copy(s):
        return remote(send.at[s], rows_in.at[me], d_send.at[s], d_recv.at[me], (s, tp))

    def d_arrival(s):
        return remote(send.at[s], rows_in.at[s], d_send.at[s], d_recv.at[s], (s, tp))

    def r_copy(j, s):
        first, count = DOWN[j]
        w = pl.ds(first, count)
        return remote(ret.at[w, s], back.at[w, me], r_send.at[j, s], r_recv.at[j, me], (s, tp))

    def r_arrival(j, s):
        first, count = DOWN[j]
        w = pl.ds(first, count)
        return remote(ret.at[w, s], back.at[w, s], r_send.at[j, s], r_recv.at[j, s], (s, tp))

    def dispatch(d, _):
        z = d
        base = pl.multiple_of(2 * z * cap, 2 * cap)
        got = jnp.dot(
            blend[pl.ds(base, 2 * cap), :], normed_out[...], preferred_element_type=jnp.float32
        ).astype(jnp.bfloat16)
        for j in range(2):
            s = 2 * z + j
            @pl.when(s != me)
            def _():
                send[s] = got[j * cap:(j + 1) * cap]
                d_copy(s).start()
            @pl.when(s == me)
            def _():
                rows_in[me] = got[j * cap:(j + 1) * cap]
        return 0

    lax.fori_loop(0, nz, dispatch, 0)

    def pass_on(p, _):
        far_piece(p).wait_recv()
        relay(p).start()
        return 0

    lax.fori_loop(0, DEEP, pass_on, 0)
    for i in range(3):
        w_copy(i).wait_recv()
    local = 2 * ff

    def gated(x, cols):
        gate = jnp.dot(x, gu[0, :, cols], preferred_element_type=jnp.float32)
        upper = jnp.dot(x, gu[1, :, cols], preferred_element_type=jnp.float32)
        return (gate / (1.0 + jnp.exp(-gate)) * upper).astype(jnp.bfloat16)

    def work(z, _):
        lax.fori_loop(DEEP + z * (DEEP // nz), DEEP + (z + 1) * (DEEP // nz), pass_on, 0)
        for j in range(2):
            s = 2 * z + j
            @pl.when(s != me)
            def _():
                d_arrival(s).wait_recv()
        x = rows_in[pl.ds(2 * z, 2)].reshape(2 * cap, d_model)
        base = pl.multiple_of(2 * z * cap, 2 * cap)
        hid[pl.ds(base, 2 * cap), :local] = gated(x, slice(0, local))
        return 0

    lax.fori_loop(0, nz, work, 0)

    def relayed(p, _):
        relay(p).wait_recv()
        return 0

    lax.fori_loop(0, 2 * DEEP, relayed, 0)
    hid[:, local:] = gated(rows_in[...].reshape(n * cap, d_model), slice(local, 2 * local))

    def give_back(j):
        far_down(j).wait_recv()
        relay_down(j).start()
        relay_down(j).wait_recv()
        first, count = DOWN[j]
        down = jnp.dot(
            hid[...], dw[:, first * wide:(first + count) * wide], preferred_element_type=jnp.float32
        ).astype(jnp.bfloat16)
        for c in range(count):
            ret[first + c] = down[:, c * wide:(c + 1) * wide].reshape(n, cap, wide)
            back[first + c, me] = ret[first + c, me]

        def one(d, _):
            for k in range(2):
                s = 2 * lax.rem(zi + d, nz) + k
                @pl.when(s != me)
                def _():
                    r_copy(j, s).start()
            return 0

        lax.fori_loop(1, nz + 1, one, 0)

    def collect(j):
        def arrive(s, _):
            @pl.when(s != me)
            def _():
                r_arrival(j, s).wait_recv()
            return 0

        lax.fori_loop(0, n, arrive, 0)
        first, count = DOWN[j]
        for c in range(first, first + count):
            results = back[c].reshape(n * cap, wide)
            routed = jnp.dot(blend_hi[...], results, preferred_element_type=jnp.float32)
            routed = routed + jnp.dot(blend_lo[...], results, preferred_element_type=jnp.float32)
            cols = slice(c * wide, (c + 1) * wide)
            out_ref[:, cols] = (stream_out[:, cols] + routed).astype(jnp.bfloat16)

    for j in range(len(DOWN)):
        give_back(j)
        if j > 1:
            collect(j - 2)
    for j in range(max(len(DOWN) - 2, 0), len(DOWN)):
        collect(j)

    finish_attention()
    for i in range(3):
        w_copy(i).wait_send()

    def passed(p, _):
        far_piece(p).wait_send()
        relay(p).wait_send()
        return 0

    lax.fori_loop(0, 2 * DEEP, passed, 0)
    for j in range(len(DOWN)):
        far_down(j).wait_send()
        relay_down(j).wait_send()

    def finish(s, _):
        @pl.when(s != me)
        def _():
            d_copy(s).wait_send()
            for j in range(len(DOWN)):
                r_copy(j, s).wait_send()
        return 0

    lax.fori_loop(0, n, finish, 0)


def layer(n, nt, cap, *args):
    q1, ow, stream_in = args[0], args[7], args[8]
    rows = q1.shape[0]
    tokens, d = stream_in.shape
    vm = pl.BlockSpec(memory_space=pltpu.VMEM)
    hbm = pl.BlockSpec(memory_space=pl.ANY)
    sm = pl.BlockSpec(memory_space=pltpu.SMEM)
    chunk = rows // nt
    dma = pltpu.SemaphoreType.DMA
    bf, f32 = jnp.bfloat16, jnp.float32
    in_specs = [hbm, hbm, hbm, hbm, hbm, sm, vm, hbm, hbm, vm]
    out_shape = (jax.ShapeDtypeStruct((tokens, d), f32), jax.ShapeDtypeStruct((tokens, d), bf))
    out_specs = (vm, vm)
    scratch = [
        pltpu.VMEM((n, rows, 2 * HEAD_DIM + VAL_DIM), bf),
        pltpu.VMEM((2, 2 * rows, HEAD_DIM), bf),
        pltpu.VMEM((2, 2 * rows, 128), f32),
        pltpu.VMEM((2, 2 * rows, 128), f32),
        pltpu.VMEM((2, 2 * rows, VAL_DIM), f32),
        pltpu.VMEM((rows, 2 * VAL_DIM), bf),
        pltpu.VMEM(ow.shape, bf),
        pltpu.VMEM((tokens, d), bf),
        pltpu.VMEM((2 * chunk, d), bf),
        pltpu.VMEM((2 * chunk, d), bf),
        pltpu.VMEM((chunk, d), bf),
        pltpu.VMEM((chunk, d), bf),
        dma((9,)), dma((n // 2 * HALVES,)), dma((n // 2 * HALVES,)), dma((n // 2 * HALVES,)), dma((n // 2 * HALVES,)), dma((2, PARTS)), dma((2, PARTS)),
    ]
    if cap:
        ff = args[12].shape[2]
        in_specs = in_specs + [vm, vm, hbm, hbm, hbm]
        out_shape = pltpu.VMEM((tokens, d), bf)
        out_specs = vm
        scratch = scratch + [
            pltpu.VMEM((tokens, d), f32),
            pltpu.VMEM((tokens, d), bf),
            pltpu.VMEM((2, d, nt * ff), bf),
            pltpu.VMEM((nt * ff, d), bf),
            pltpu.VMEM((n * cap, tokens), bf),
            pltpu.VMEM((tokens, n * cap), bf),
            pltpu.VMEM((tokens, n * cap), bf),
        ] + [pltpu.VMEM((n, cap, d), bf)] * 2 + [
            pltpu.VMEM((n * cap, nt * ff), bf),
            pltpu.VMEM((WIDE, n, cap, d // WIDE), bf),
            pltpu.VMEM((WIDE, n, cap, d // WIDE), bf),
            pltpu.SemaphoreType.REGULAR((2,)), dma((3,)), dma((3,)), dma((3,)),
        ] + [dma((2 * DEEP + len(DOWN),))] * 4 + [dma((n,))] * 2 + [dma((len(DOWN), n))] * 2
    return pl.pallas_call(
        functools.partial(layer_kernel, n, nt, cap),
        out_shape=out_shape,
        in_specs=in_specs,
        out_specs=out_specs,
        scratch_shapes=scratch,
        compiler_params=pltpu.CompilerParams(
            collective_id=0, has_side_effects=True, vmem_limit_bytes=58 * 2**20
        ),
        name="layer",
    )(*args)


def shards(
    stream_in,
    queries_one,
    queries_two,
    keys_one,
    keys_two,
    values,
    lambdas,
    head_gain,
    out_weight,
    norm_gain,
    expert_ids,
    route_weight,
    gate_weight,
    up_weight,
    down_weight,
):
    n, nt = lax.axis_size("sp"), lax.axis_size("tp")
    rows_here = stream_in.shape[0]
    top_count = expert_ids.shape[1]
    slot_cap = 2 * top_count * rows_here // n
    shared = (
        queries_one, queries_two, keys_one, keys_two, values, lambdas,
        head_gain.reshape(1, -1), out_weight, stream_in, norm_gain.reshape(1, -1),
    )
    if slot_cap % 16 == 0:
        return layer(
            n, nt, slot_cap, *shared, expert_ids.T, route_weight.T, gate_weight, up_weight, down_weight
        )
    stream, normed = layer(n, nt, 0, *shared)
    flat_ids = expert_ids.reshape(-1)
    count = flat_ids.shape[0]
    order = lax.iota(jnp.int32, count)
    earlier = (flat_ids[None, :] == flat_ids[:, None]) & (order[None, :] < order[:, None])
    ranks = jnp.sum(earlier.astype(jnp.int32), axis=1)
    slots = flat_ids * slot_cap + ranks
    slot_of = slots.reshape(rows_here, top_count)
    places = lax.iota(jnp.int32, n * slot_cap)
    selector = sum(
        (slot_of[:, k][None, :] == places[:, None]).astype(jnp.bfloat16) for k in range(top_count)
    )
    send_rows = jnp.dot(selector, normed, preferred_element_type=jnp.float32).astype(jnp.bfloat16)
    received = lax.all_to_all(send_rows, "sp", split_axis=0, concat_axis=0, tiled=True)
    picked_rows = lax.all_gather(received, "tp", axis=0, tiled=True)
    gate = jnp.dot(picked_rows, gate_weight[0], preferred_element_type=jnp.float32)
    upper = jnp.dot(picked_rows, up_weight[0], preferred_element_type=jnp.float32)
    hidden = (jax.nn.silu(gate) * upper).astype(jnp.bfloat16)
    summed = lax.psum_scatter(
        jnp.dot(hidden, down_weight[0], preferred_element_type=jnp.float32).astype(jnp.bfloat16),
        "tp",
        scatter_dimension=0,
        tiled=True,
    )
    returned = lax.all_to_all(summed, "sp", split_axis=0, concat_axis=0, tiled=True)
    picked = jnp.take(returned, slots, axis=0).reshape(rows_here, top_count, -1).astype(jnp.float32)
    routed = jnp.sum(picked * route_weight[:, :, None], axis=1)
    return (stream + routed).astype(jnp.bfloat16)


def solution(mesh):
    return jax.shard_map(
        shards,
        mesh=mesh,
        in_specs=(
            P(("sp", "tp"), None),
            P("sp", "tp"),
            P("sp", "tp"),
            P("sp", "tp"),
            P("sp", "tp"),
            P("sp", "tp"),
            P("tp"),
            P(),
            P("tp", None),
            P(),
            P(("sp", "tp"), None),
            P(("sp", "tp"), None),
            P("sp", None, "tp"),
            P("sp", None, "tp"),
            P("sp", "tp", None),
        ),
        out_specs=P(("sp", "tp"), None),
        check_vma=False,
    )
```

```python
import functools

import jax
import jax.numpy as jnp
from jax import lax
from jax.experimental import pallas as pl
from jax.experimental.pallas import tpu as pltpu
from jax.sharding import PartitionSpec as P

HEAD_DIM = 128
VAL_DIM = 256


EPS = 1e-06
OUT_SCALE = 0.8


MESH = pl.DeviceIdType.MESH
LOG2E = 1.4426950408889634
DEEP = 8
WIDE = 8
DOWN = ((0, 1), (1, 1), (2, 1), (3, 1), (4, 1), (5, 1), (6, 1), (7, 1))
PARTS = 4
HALVES = 2


def remote(src, dst, send_sem, recv_sem, where):
    return pltpu.make_async_remote_copy(
        src_ref=src,
        dst_ref=dst,
        send_sem=send_sem,
        recv_sem=recv_sem,
        device_id=where,
        device_id_type=MESH,
    )


def greet(devices, count):
    barrier = pltpu.get_barrier_semaphore()
    devices(lambda where: pl.semaphore_signal(barrier, inc=1, device_id=where, device_id_type=MESH))
    pl.semaphore_wait(barrier, count)


def layer_kernel(n, nt, cap, *refs):
    (
        q1_ref, q2_ref, k1_ref, k2_ref, v_ref, lam_ref, gain_ref, ow_ref, stream_ref, norm_ref,
    ) = refs[:10]
    if cap:
        ids_ref, route_ref, gw_ref, uw_ref, dw_ref, out_ref = refs[10:16]
        refs = refs[16:]
    else:
        stream_out, normed_out = refs[10:12]
        refs = refs[12:]
    kv, qs, top, total, acc, heads, ow, stream, near_part, near_got, far_part, far_got = refs[:12]
    local_sem, z_send, z_recv, y_send, y_recv, p_send, p_recv = refs[12:19]
    if cap:
        (
            stream_out, normed_out, gu, dw, blend, blend_back, send, rows_in, hid, ret, back,
            chain, own_sem, w_send, w_recv, f_send, f_recv, g_send, g_recv, d_send, d_recv, r_send, r_recv,
        ) = refs[19:]

    me, tp = lax.axis_index("sp"), lax.axis_index("tp")
    nz = n // 2
    zi, y = me // 2, lax.rem(me, 2)
    pair = me + 1 - 2 * y
    rows = q1_ref.shape[0]
    hd = HEAD_DIM
    chunk = rows // nt
    side, core = tp // 2, lax.rem(tp, 2)
    near = (me, tp + 1 - 2 * core)
    far = (me, lax.rem(tp + 2, 4))

    loads = [
        pltpu.make_async_copy(k1_ref, kv.at[me, :, pl.ds(0, hd)], local_sem.at[0]),
        pltpu.make_async_copy(k2_ref, kv.at[me, :, pl.ds(hd, hd)], local_sem.at[1]),
        pltpu.make_async_copy(v_ref, kv.at[me, :, pl.ds(2 * hd, VAL_DIM)], local_sem.at[2]),
    ]
    rest = [
        pltpu.make_async_copy(
            ref.at[:, pl.ds(h * hd, hd)], qs.at[i, pl.ds(h * rows, rows), :], local_sem.at[4 + 2 * i + h]
        )
        for i, ref in enumerate((q1_ref, q2_ref))
        for h in range(2)
    ]
    stream_load = pltpu.make_async_copy(stream_ref, stream, local_sem.at[8])
    for load in loads + rest:
        load.start()
    stream_load.start()
    if cap:
        ff = gw_ref.shape[2]

        deep = gu.shape[1] // DEEP
        wide = dw.shape[1] // WIDE

        def part_of(i, k):
            if i == 2:
                return dw.at[pl.ds(k * ff, ff), :]
            return gu.at[i, :, pl.ds(k * ff, ff)]

        own_loads = [
            pltpu.make_async_copy(ref.at[0], part_of(i, 0), own_sem.at[i])
            for i, ref in enumerate((gw_ref, uw_ref, dw_ref))
        ]
        for load in own_loads:
            load.start()

        def w_copy(i):
            return remote(part_of(i, 0), part_of(i, 1), w_send.at[0], w_recv.at[0], near)

        def piece(p, k):
            rows_of = pl.ds(pl.multiple_of(lax.rem(p, DEEP) * deep, deep), deep)
            return gu.at[p // DEEP, rows_of, pl.ds(k * ff, ff)]

        def far_piece(p):
            return remote(piece(p, 0), piece(p, 2), f_send.at[0], f_recv.at[p], far)

        def relay(p):
            return remote(piece(p, 2), piece(p, 3), g_send.at[0], g_recv.at[0], near)

        def down_piece(j, k):
            first, count = DOWN[j]
            return dw.at[pl.ds(k * ff, ff), pl.ds(first * wide, count * wide)]

        def far_down(j):
            p = 2 * DEEP + j
            return remote(down_piece(j, 0), down_piece(j, 2), f_send.at[0], f_recv.at[p], far)

        def relay_down(j):
            return remote(down_piece(j, 2), down_piece(j, 3), g_send.at[0], g_recv.at[1 + j], near)

        def third(k):
            return dw.at[pl.ds(k, 3 * ff), :]

        ahead = jnp.minimum(jnp.where(zi == 0, 5, jnp.where(zi == nz - 1, 10, 6 + zi)), 2 * DEEP)

        def far_some(p, _):
            far_piece(p).start()
            return 0

    ow_load = pltpu.make_async_copy(ow_ref, ow, local_sem.at[3])
    ow_load.start()

    below, above = zi > 0, zi < nz - 1

    def peers(tell):
        tell(near)
        tell(far)
        tell((pair, tp))
        @pl.when(below)
        def _():
            tell((me - 2, tp))
        @pl.when(above)
        def _():
            tell((me + 2, tp))

    greet(peers, 3 + below.astype(jnp.int32) + above.astype(jnp.int32))
    for load in loads:
        load.wait()

    part_rows = rows // HALVES

    def block(b, c):
        return kv.at[b, pl.ds(c * part_rows, part_rows), :]

    def hop(z, c):
        b, i = 2 * z + y, HALVES * z + c
        return remote(block(b, c), block(b, c), z_send.at[i], z_recv.at[i], (jnp.minimum(me + 2, n - 2 + y), tp))

    def y_copy(z, c):
        b, i = 2 * z + y, HALVES * z + c
        return remote(block(b, c), block(b, c), y_send.at[i], y_recv.at[i], (pair, tp))

    def y_arrival(z, c):
        b, i = 2 * z + 1 - y, HALVES * z + c
        return remote(block(b, c), block(b, c), y_send.at[i], y_recv.at[i], (pair, tp))

    for c in range(HALVES):
        @pl.when(zi < nz - 1)
        def _():
            hop(zi, c).start()

        @pl.when(y == 0)
        def _():
            y_copy(zi, c).start()

    if cap:
        own_loads[0].wait()
        own_loads[1].wait()
        lax.fori_loop(0, ahead, far_some, 0)
        own_loads[2].wait()
        for i in range(3):
            w_copy(i).start()

    for load in rest:
        load.wait()

    scale = HEAD_DIM ** (-0.5) * LOG2E

    def fold(b, first):
        vals = kv[b, :, 2 * hd:]
        for i in range(2):
            keys = kv[b, :, i * hd:(i + 1) * hd]
            s = lax.dot_general(qs[i], keys, (((1,), (1,)), ((), ())), preferred_element_type=jnp.float32)
            if first:
                r = lax.broadcasted_iota(jnp.int32, (2, rows, rows), 1).reshape(2 * rows, rows)
                c = lax.broadcasted_iota(jnp.int32, (2 * rows, rows), 1)
                s = jnp.where(c <= r, s, -jnp.inf)
            new = jnp.broadcast_to(jnp.max(s, axis=-1, keepdims=True), (2 * rows, 128))
            if not first:
                old = top[i]
                new = jnp.maximum(old, new)
            terms = [jnp.exp2((s[:, c:c + 128] - new) * scale) for c in range(0, rows, 128)]
            weights = jnp.concatenate([e.astype(jnp.bfloat16) for e in terms], axis=1)
            pv = jnp.dot(weights, vals, preferred_element_type=jnp.float32)
            if first:
                acc[i] = pv
                total[i] = sum(terms)
            else:
                alpha = jnp.exp2((old - new) * scale)
                for c in range(0, VAL_DIM, 128):
                    acc[i, :, c:c + 128] = acc[i, :, c:c + 128] * alpha + pv[:, c:c + 128]
                total[i] = total[i] * alpha + sum(terms)
            top[i] = new

    fold(me, True)

    ways = ((0, above, below, me - 2), (1, below, above, me + 2))

    def tell_on(i, where):
        pl.semaphore_signal(chain.at[i], inc=1, device_id=(where, tp), device_id_type=MESH)

    if cap:
        for i, source, target, where in ways:
            @pl.when(jnp.logical_and(jnp.logical_not(source), target))
            def _():
                tell_on(i, where)

    if cap:
        choices, tokens = ids_ref.shape
        which = lax.broadcasted_iota(jnp.int32, (max(n, 8), tokens), 0)
        named = [(ids_ref[k:k + 1, :] == which).astype(jnp.float32) for k in range(choices)]
        before = lax.broadcasted_iota(jnp.int32, (tokens, tokens), 0) < lax.broadcasted_iota(
            jnp.int32, (tokens, tokens), 1
        )
        counts = jnp.dot(
            sum(named).astype(jnp.bfloat16), before.astype(jnp.bfloat16), preferred_element_type=jnp.float32
        )
        place = lax.broadcasted_iota(jnp.int32, (n * cap, tokens), 0)
        chosen = jnp.zeros((n * cap, tokens), jnp.float32)
        weight = jnp.zeros((n * cap, tokens), jnp.float32)
        for k in range(choices):
            rank = jnp.sum(named[k] * counts, axis=0, keepdims=True).astype(jnp.int32)
            hit = (ids_ref[k:k + 1, :] * cap + rank) == place
            chosen = chosen + hit.astype(jnp.float32)
            weight = weight + jnp.where(hit, route_ref[k:k + 1, :], 0.0)
        blend[...] = chosen.astype(jnp.bfloat16)
        weight = weight.T
        coarse = weight.astype(jnp.bfloat16)
        blend_back[:tokens] = coarse
        blend_back[tokens:] = (weight - coarse.astype(jnp.float32)).astype(jnp.bfloat16)

    def walk(d, _):
        z = zi - d
        @pl.when(d <= zi)
        def _():
            for c in range(HALVES):
                hop(z, c).wait_recv()
                y_copy(z, c).start()
                @pl.when(zi < nz - 1)
                def _():
                    hop(z, c).start()
            fold(2 * z + y, False)
        @pl.when(jnp.logical_or(d > 1, y == 1))
        def _():
            for c in range(HALVES):
                y_arrival(z + 1, c).wait_recv()
            fold(2 * (z + 1) + 1 - y, False)
        if cap:
            @pl.when((d == 1) & below & above)
            def _():
                for i, _, _, where in ways:
                    pl.semaphore_wait(chain.at[i], 1)
                    tell_on(i, where)
        return 0

    lax.fori_loop(1, jnp.where(zi + y > 0, zi + 2, 1), walk, 0)

    for h in range(2):
        r = pl.ds(h * rows, rows)
        one = acc[0, r, :] / jnp.sum(total[0, r, :], axis=-1, keepdims=True)
        two = acc[1, r, :] / jnp.sum(total[1, r, :], axis=-1, keepdims=True)
        diff = one - lam_ref[h] * two
        ms = jnp.mean(diff * diff, axis=-1, keepdims=True)
        heads[:, h * VAL_DIM:(h + 1) * VAL_DIM] = (
            diff * lax.rsqrt(ms + EPS) * gain_ref[...] * OUT_SCALE
        ).astype(jnp.bfloat16)

    ow_load.wait()

    d_model = ow.shape[1]
    span = d_model // PARTS

    def picked(first, second):
        return jnp.concatenate(
            [heads[pl.ds(pl.multiple_of(t * chunk, chunk), chunk), :] for t in (first, second)], axis=0
        )

    def near_copy(q):
        cols = pl.ds(q * span, span)
        return remote(near_part.at[:, cols], near_got.at[:, cols], p_send.at[0], p_recv.at[0, q], near)

    def far_copy(q):
        cols = pl.ds(q * span, span)
        return remote(far_part.at[:, cols], far_got.at[:, cols], p_send.at[1], p_recv.at[1, q], far)

    away = 1 - side
    other = picked(2 * away + 1 - core, 2 * side + 1 - core)
    for q in range(PARTS):
        cols = slice(q * span, (q + 1) * span)
        near_part[:, cols] = jnp.dot(
            other, ow[:, cols], preferred_element_type=jnp.float32
        ).astype(jnp.bfloat16)
        near_copy(q).start()
    stream_load.wait()
    own = picked(2 * away + core, 2 * side + core)
    for q in range(PARTS):
        cols = slice(q * span, (q + 1) * span)
        mine = jnp.dot(own, ow[:, cols], preferred_element_type=jnp.float32)
        near_copy(q).wait_recv()
        mine = mine + near_got[:, cols].astype(jnp.float32)
        far_part[:, cols] = mine[:chunk].astype(jnp.bfloat16)
        far_copy(q).start()
        stream_out[:, cols] = stream[:, cols].astype(jnp.float32) + mine[chunk:]
    if cap:
        lax.fori_loop(ahead, 2 * DEEP, far_some, 0)
        for j in range(len(DOWN)):
            far_down(j).start()
    square = jnp.zeros((chunk, 1), jnp.float32)
    for q in range(PARTS):
        cols = slice(q * span, (q + 1) * span)
        far_copy(q).wait_recv()
        summed = stream_out[:, cols] + far_got[:, cols].astype(jnp.float32)
        stream_out[:, cols] = summed
        square = square + jnp.sum(summed * summed, axis=-1, keepdims=True)
    normed_out[...] = (
        stream_out[...] * lax.rsqrt(square * (1.0 / d_model) + EPS) * norm_ref[...]
    ).astype(jnp.bfloat16)

    def finish_attention():
        remote(near_part, near_got, p_send.at[0], p_recv.at[0, 0], near).wait_send()
        remote(far_part, far_got, p_send.at[1], p_recv.at[1, 0], far).wait_send()

        for c in range(HALVES):
            @pl.when(y == 0)
            def _():
                y_copy(zi, c).wait_send()

            @pl.when(zi < nz - 1)
            def _():
                hop(zi, c).wait_send()

        def sent(z, _):
            for c in range(HALVES):
                y_copy(z, c).wait_send()
                @pl.when(zi < nz - 1)
                def _():
                    hop(z, c).wait_send()
            return 0

        lax.fori_loop(0, zi, sent, 0)

    if not cap:
        finish_attention()
        return

    def d_copy(s):
        return remote(send.at[s], rows_in.at[me], d_send.at[0], d_recv.at[zi], (s, tp))

    def d_arrival(first, count):
        some = pl.ds(first, count)
        return remote(send.at[some], rows_in.at[some], d_send.at[0], d_recv.at[first // 2], (pair, tp))

    def r_copy(j, s):
        first, count = DOWN[j]
        w = pl.ds(first, count)
        return remote(ret.at[w, s], back.at[w, me], r_send.at[0], r_recv.at[j], (s, tp))

    others = pl.ds(0, n - 1)

    def r_arrival(j):
        first, count = DOWN[j]
        w = pl.ds(first, count)
        return remote(ret.at[w, others], back.at[w, others], r_send.at[0], r_recv.at[j], (pair, tp))

    def dispatch(d, _):
        z = d
        base = pl.multiple_of(2 * z * cap, 2 * cap)
        got = jnp.dot(
            blend[pl.ds(base, 2 * cap), :], normed_out[...], preferred_element_type=jnp.float32
        ).astype(jnp.bfloat16)
        for j in range(2):
            s = 2 * z + j
            @pl.when(s != me)
            def _():
                send[s] = got[j * cap:(j + 1) * cap]
                d_copy(s).start()
            @pl.when(s == me)
            def _():
                rows_in[me] = got[j * cap:(j + 1) * cap]
        return 0

    for i, source, target, _ in ways:
        @pl.when(jnp.logical_and(source, jnp.logical_not(target)))
        def _():
            pl.semaphore_wait(chain.at[i], 1)
    lax.fori_loop(0, nz, dispatch, 0)

    def pass_on(p, _):
        far_piece(p).wait_recv()
        relay(p).start()
        return 0

    lax.fori_loop(0, DEEP, pass_on, 0)
    remote(third(0), third(ff), w_send.at[0], w_recv.at[0], near).wait_recv()
    local = 2 * ff

    def gated(x, cols):
        gate = jnp.dot(x, gu[0, :, cols], preferred_element_type=jnp.float32)
        upper = jnp.dot(x, gu[1, :, cols], preferred_element_type=jnp.float32)
        return (gate / (1.0 + jnp.exp(-gate)) * upper).astype(jnp.bfloat16)

    def work(z, _):
        lax.fori_loop(DEEP + z * (DEEP // nz), DEEP + (z + 1) * (DEEP // nz), pass_on, 0)
        @pl.when(z != zi)
        def _():
            d_arrival(2 * z, 2).wait_recv()
        @pl.when(z == zi)
        def _():
            d_arrival(pair, 1).wait_recv()
        x = rows_in[pl.ds(2 * z, 2)].reshape(2 * cap, d_model)
        base = pl.multiple_of(2 * z * cap, 2 * cap)
        hid[pl.ds(base, 2 * cap), :local] = gated(x, slice(0, local))
        return 0

    lax.fori_loop(0, nz, work, 0)

    ends = gu.at[:, :, pl.ds(3 * ff, ff)]
    remote(ends, ends, g_send.at[0], g_recv.at[0], near).wait_recv()
    hid[:, local:] = gated(rows_in[...].reshape(n * cap, d_model), slice(local, 2 * local))

    def give_back(j):
        far_down(j).wait_recv()
        relay_down(j).start()
        relay_down(j).wait_recv()
        first, count = DOWN[j]
        down = jnp.dot(
            hid[...], dw[:, first * wide:(first + count) * wide], preferred_element_type=jnp.float32
        ).astype(jnp.bfloat16)
        for c in range(count):
            ret[first + c] = down[:, c * wide:(c + 1) * wide].reshape(n, cap, wide)
            back[first + c, me] = ret[first + c, me]

        def one(d, _):
            for k in range(2):
                s = 2 * jnp.where(zi >= nz // 2, d, nz - 1 - d) + k
                @pl.when(s != me)
                def _():
                    r_copy(j, s).start()
            return 0

        lax.fori_loop(0, nz, one, 0)

    def collect(j):
        r_arrival(j).wait_recv()
        first, count = DOWN[j]
        results = jnp.concatenate(
            [back[c].reshape(n * cap, wide) for c in range(first, first + count)], axis=1
        )
        routed = jnp.dot(blend_back[...], results, preferred_element_type=jnp.float32)
        cols = slice(first * wide, (first + count) * wide)
        out_ref[:, cols] = (stream_out[:, cols] + routed[:tokens] + routed[tokens:]).astype(jnp.bfloat16)

    for j in range(len(DOWN)):
        give_back(j)
        if j > 1:
            collect(j - 2)
    finish_attention()
    remote(third(0), third(ff), w_send.at[0], w_recv.at[0], near).wait_send()
    remote(third(0), third(ff), f_send.at[0], f_recv.at[0], far).wait_send()
    remote(third(0), third(ff), g_send.at[0], g_recv.at[0], near).wait_send()
    remote(send.at[others], rows_in.at[others], d_send.at[0], d_recv.at[0], (pair, tp)).wait_send()
    remote(ret.at[:, others], back.at[:, others], r_send.at[0], r_recv.at[0], (pair, tp)).wait_send()

    for j in range(max(len(DOWN) - 2, 0), len(DOWN)):
        collect(j)


def layer(n, nt, cap, *args):
    q1, ow, stream_in = args[0], args[7], args[8]
    rows = q1.shape[0]
    tokens, d = stream_in.shape
    vm = pl.BlockSpec(memory_space=pltpu.VMEM)
    hbm = pl.BlockSpec(memory_space=pl.ANY)
    sm = pl.BlockSpec(memory_space=pltpu.SMEM)
    chunk = rows // nt
    dma = pltpu.SemaphoreType.DMA
    bf, f32 = jnp.bfloat16, jnp.float32
    in_specs = [hbm, hbm, hbm, hbm, hbm, sm, vm, hbm, hbm, vm]
    out_shape = (jax.ShapeDtypeStruct((tokens, d), f32), jax.ShapeDtypeStruct((tokens, d), bf))
    out_specs = (vm, vm)
    scratch = [
        pltpu.VMEM((n, rows, 2 * HEAD_DIM + VAL_DIM), bf),
        pltpu.VMEM((2, 2 * rows, HEAD_DIM), bf),
        pltpu.VMEM((2, 2 * rows, 128), f32),
        pltpu.VMEM((2, 2 * rows, 128), f32),
        pltpu.VMEM((2, 2 * rows, VAL_DIM), f32),
        pltpu.VMEM((rows, 2 * VAL_DIM), bf),
        pltpu.VMEM(ow.shape, bf),
        pltpu.VMEM((tokens, d), bf),
        pltpu.VMEM((2 * chunk, d), bf),
        pltpu.VMEM((2 * chunk, d), bf),
        pltpu.VMEM((chunk, d), bf),
        pltpu.VMEM((chunk, d), bf),
        dma((9,)), dma((n // 2 * HALVES,)), dma((n // 2 * HALVES,)), dma((n // 2 * HALVES,)), dma((n // 2 * HALVES,)), dma((2,)), dma((2, PARTS)),
    ]
    if cap:
        ff = args[12].shape[2]
        in_specs = in_specs + [vm, vm, hbm, hbm, hbm]
        out_shape = pltpu.VMEM((tokens, d), bf)
        out_specs = vm
        scratch = scratch + [
            pltpu.VMEM((tokens, d), f32),
            pltpu.VMEM((tokens, d), bf),
            pltpu.VMEM((2, d, nt * ff), bf),
            pltpu.VMEM((nt * ff, d), bf),
            pltpu.VMEM((n * cap, tokens), bf),
            pltpu.VMEM((2 * tokens, n * cap), bf),
        ] + [pltpu.VMEM((n, cap, d), bf)] * 2 + [
            pltpu.VMEM((n * cap, nt * ff), bf),
            pltpu.VMEM((WIDE, n, cap, d // WIDE), bf),
            pltpu.VMEM((WIDE, n, cap, d // WIDE), bf),
            pltpu.SemaphoreType.REGULAR((2,)), dma((3,)), dma((1,)), dma((1,)),
        ] + [
            dma((1,)), dma((2 * DEEP + len(DOWN),)), dma((1,)), dma((1 + len(DOWN),)),
            dma((1,)), dma((n // 2,)), dma((1,)), dma((len(DOWN),)),
        ]
    return pl.pallas_call(
        functools.partial(layer_kernel, n, nt, cap),
        out_shape=out_shape,
        in_specs=in_specs,
        out_specs=out_specs,
        scratch_shapes=scratch,
        compiler_params=pltpu.CompilerParams(
            collective_id=0, has_side_effects=True, vmem_limit_bytes=58 * 2**20
        ),
        name="layer",
    )(*args)


def shards(
    stream_in,
    queries_one,
    queries_two,
    keys_one,
    keys_two,
    values,
    lambdas,
    head_gain,
    out_weight,
    norm_gain,
    expert_ids,
    route_weight,
    gate_weight,
    up_weight,
    down_weight,
):
    n, nt = lax.axis_size("sp"), lax.axis_size("tp")
    rows_here = stream_in.shape[0]
    top_count = expert_ids.shape[1]
    slot_cap = 2 * top_count * rows_here // n
    shared = (
        queries_one, queries_two, keys_one, keys_two, values, lambdas,
        head_gain.reshape(1, -1), out_weight, stream_in, norm_gain.reshape(1, -1),
    )
    if slot_cap % 16 == 0:
        return layer(
            n, nt, slot_cap, *shared, expert_ids.T, route_weight.T, gate_weight, up_weight, down_weight
        )
    stream, normed = layer(n, nt, 0, *shared)
    flat_ids = expert_ids.reshape(-1)
    count = flat_ids.shape[0]
    order = lax.iota(jnp.int32, count)
    earlier = (flat_ids[None, :] == flat_ids[:, None]) & (order[None, :] < order[:, None])
    ranks = jnp.sum(earlier.astype(jnp.int32), axis=1)
    slots = flat_ids * slot_cap + ranks
    slot_of = slots.reshape(rows_here, top_count)
    places = lax.iota(jnp.int32, n * slot_cap)
    selector = sum(
        (slot_of[:, k][None, :] == places[:, None]).astype(jnp.bfloat16) for k in range(top_count)
    )
    send_rows = jnp.dot(selector, normed, preferred_element_type=jnp.float32).astype(jnp.bfloat16)
    received = lax.all_to_all(send_rows, "sp", split_axis=0, concat_axis=0, tiled=True)
    picked_rows = lax.all_gather(received, "tp", axis=0, tiled=True)
    gate = jnp.dot(picked_rows, gate_weight[0], preferred_element_type=jnp.float32)
    upper = jnp.dot(picked_rows, up_weight[0], preferred_element_type=jnp.float32)
    hidden = (jax.nn.silu(gate) * upper).astype(jnp.bfloat16)
    summed = lax.psum_scatter(
        jnp.dot(hidden, down_weight[0], preferred_element_type=jnp.float32).astype(jnp.bfloat16),
        "tp",
        scatter_dimension=0,
        tiled=True,
    )
    returned = lax.all_to_all(summed, "sp", split_axis=0, concat_axis=0, tiled=True)
    picked = jnp.take(returned, slots, axis=0).reshape(rows_here, top_count, -1).astype(jnp.float32)
    routed = jnp.sum(picked * route_weight[:, :, None], axis=1)
    return (stream + routed).astype(jnp.bfloat16)


def solution(mesh):
    return jax.shard_map(
        shards,
        mesh=mesh,
        in_specs=(
            P(("sp", "tp"), None),
            P("sp", "tp"),
            P("sp", "tp"),
            P("sp", "tp"),
            P("sp", "tp"),
            P("sp", "tp"),
            P("tp"),
            P(),
            P("tp", None),
            P(),
            P(("sp", "tp"), None),
            P(("sp", "tp"), None),
            P("sp", None, "tp"),
            P("sp", None, "tp"),
            P("sp", "tp", None),
        ),
        out_specs=P(("sp", "tp"), None),
        check_vma=False,
    )
```

```python
import functools

import jax
import jax.numpy as jnp
from jax import lax
from jax.experimental import pallas as pl
from jax.experimental.pallas import tpu as pltpu
from jax.sharding import PartitionSpec as P

HEAD_DIM = 128
VAL_DIM = 256


EPS = 1e-06
OUT_SCALE = 0.8


MESH = pl.DeviceIdType.MESH
LOG2E = 1.4426950408889634
DEEP = 8
WIDE = 16
DOWN = ((0, 2), (2, 2), (4, 2), (6, 2), (8, 2), (10, 2), (12, 2), (14, 2))
PARTS = 4
HALVES = 2


def remote(src, dst, send_sem, recv_sem, where):
    return pltpu.make_async_remote_copy(
        src_ref=src,
        dst_ref=dst,
        send_sem=send_sem,
        recv_sem=recv_sem,
        device_id=where,
        device_id_type=MESH,
    )


def greet(devices, count):
    barrier = pltpu.get_barrier_semaphore()
    devices(lambda where: pl.semaphore_signal(barrier, inc=1, device_id=where, device_id_type=MESH))
    pl.semaphore_wait(barrier, count)


def layer_kernel(n, nt, cap, *refs):
    (
        q1_ref, q2_ref, k1_ref, k2_ref, v_ref, lam_ref, gain_ref, ow_ref, stream_ref, norm_ref,
    ) = refs[:10]
    if cap:
        ids_ref, route_ref, gw_ref, uw_ref, dw_ref, out_ref = refs[10:16]
        refs = refs[16:]
    else:
        stream_out, normed_out = refs[10:12]
        refs = refs[12:]
    kv, qs, top, total, acc, heads, ow, stream, lam, gain, norm, near_part, near_got, far_part, far_got = refs[:15]
    local_sem, z_send, z_recv, y_send, y_recv, p_send, p_recv = refs[15:22]
    if cap:
        (
            stream_out, normed_out, gu, dw, blend, blend_back, send, rows_in, hid,
            ids, route, chain, own_sem, w_send, w_recv, f_send, f_recv, g_send, g_recv, d_send, d_recv, r_send, r_recv,
        ) = refs[22:-2 * len(DOWN)]
        ret, back = refs[-2 * len(DOWN):-len(DOWN)], refs[-len(DOWN):]

    me, tp = lax.axis_index("sp"), lax.axis_index("tp")
    nz = n // 2
    zi, y = me // 2, lax.rem(me, 2)
    pair = me + 1 - 2 * y
    rows = q1_ref.shape[0]
    hd = HEAD_DIM
    chunk = rows // nt
    side, core = tp // 2, lax.rem(tp, 2)
    near = (me, tp + 1 - 2 * core)
    far = (me, lax.rem(tp + 2, 4))

    loads = [
        pltpu.make_async_copy(k1_ref, kv.at[me, :, pl.ds(0, hd)], local_sem.at[0]),
        pltpu.make_async_copy(k2_ref, kv.at[me, :, pl.ds(hd, hd)], local_sem.at[1]),
        pltpu.make_async_copy(v_ref, kv.at[me, :, pl.ds(2 * hd, VAL_DIM)], local_sem.at[2]),
    ]
    rest = [
        pltpu.make_async_copy(
            ref.at[:, pl.ds(h * hd, hd)], qs.at[i, pl.ds(h * rows, rows), :], local_sem.at[4 + 2 * i + h]
        )
        for i, ref in enumerate((q1_ref, q2_ref))
        for h in range(2)
    ]
    stream_load = pltpu.make_async_copy(stream_ref, stream, local_sem.at[8])
    small = [(lam_ref, lam), (gain_ref, gain), (norm_ref, norm)]
    if cap:
        small = small + [(ids_ref, ids), (route_ref, route)]
    small_loads = [
        pltpu.make_async_copy(ref, held, local_sem.at[9 + i]) for i, (ref, held) in enumerate(small)
    ]
    for load in loads + rest:
        load.start()
    stream_load.start()
    for load in small_loads:
        load.start()
    if cap:
        ff = gw_ref.shape[2]

        deep = gu.shape[1] // DEEP
        wide = dw.shape[1] // WIDE

        def part_of(i, k):
            if i == 2:
                return dw.at[pl.ds(k * ff, ff), :]
            return gu.at[i, :, pl.ds(k * ff, ff)]

        own_loads = [
            pltpu.make_async_copy(ref.at[0], part_of(i, 0), own_sem.at[i])
            for i, ref in enumerate((gw_ref, uw_ref, dw_ref))
        ]
        for load in own_loads:
            load.start()

        def w_copy(i):
            return remote(part_of(i, 0), part_of(i, 1), w_send.at[0], w_recv.at[0], near)

        def piece(p, k):
            rows_of = pl.ds(pl.multiple_of(lax.rem(p, DEEP) * deep, deep), deep)
            return gu.at[p // DEEP, rows_of, pl.ds(k * ff, ff)]

        def far_piece(p):
            return remote(piece(p, 0), piece(p, 2), f_send.at[0], f_recv.at[p], far)

        def relay(p):
            return remote(piece(p, 2), piece(p, 3), g_send.at[0], g_recv.at[p // DEEP], near)

        def down_piece(j, k):
            first, count = DOWN[j]
            return dw.at[pl.ds(k * ff, ff), pl.ds(first * wide, count * wide)]

        def far_down(j):
            p = 2 * DEEP + j
            return remote(down_piece(j, 0), down_piece(j, 2), f_send.at[0], f_recv.at[p], far)

        def relay_down(j):
            return remote(down_piece(j, 2), down_piece(j, 3), g_send.at[0], g_recv.at[2 + j], near)

        def third(k):
            return dw.at[pl.ds(k, 3 * ff), :]

        ahead = jnp.minimum(jnp.where(zi == 0, 5, jnp.where(zi == nz - 1, 10, 6 + zi)), 2 * DEEP)

        def far_some(p, _):
            far_piece(p).start()
            return 0

    ow_load = pltpu.make_async_copy(ow_ref, ow, local_sem.at[3])
    ow_load.start()

    below, above = zi > 0, zi < nz - 1

    def peers(tell):
        tell(near)
        tell(far)
        tell((pair, tp))
        @pl.when(below)
        def _():
            tell((me - 2, tp))
        @pl.when(above)
        def _():
            tell((me + 2, tp))

    greet(peers, 3 + below.astype(jnp.int32) + above.astype(jnp.int32))
    for load in loads:
        load.wait()

    part_rows = rows // HALVES

    def block(b, c):
        return kv.at[b, pl.ds(c * part_rows, part_rows), :]

    def hop(z, c):
        b, i = 2 * z + y, HALVES * z + c
        return remote(block(b, c), block(b, c), z_send.at[i], z_recv.at[i], (jnp.minimum(me + 2, n - 2 + y), tp))

    def y_copy(z, c):
        b, i = 2 * z + y, HALVES * z + c
        return remote(block(b, c), block(b, c), y_send.at[i], y_recv.at[i], (pair, tp))

    def y_arrival(z, c):
        b, i = 2 * z + 1 - y, HALVES * z + c
        return remote(block(b, c), block(b, c), y_send.at[i], y_recv.at[i], (pair, tp))

    for c in range(HALVES):
        @pl.when(zi < nz - 1)
        def _():
            hop(zi, c).start()

        @pl.when(y == 0)
        def _():
            y_copy(zi, c).start()

    if cap:
        own_loads[0].wait()
        own_loads[1].wait()
        lax.fori_loop(0, ahead, far_some, 0)
        own_loads[2].wait()
        for i in range(3):
            w_copy(i).start()

    for load in rest + small_loads:
        load.wait()

    scale = HEAD_DIM ** (-0.5) * LOG2E

    def fold(b, first):
        vals = kv[b, :, 2 * hd:]
        for i in range(2):
            keys = kv[b, :, i * hd:(i + 1) * hd]
            s = lax.dot_general(qs[i], keys, (((1,), (1,)), ((), ())), preferred_element_type=jnp.float32)
            if first:
                r = lax.broadcasted_iota(jnp.int32, (2, rows, rows), 1).reshape(2 * rows, rows)
                c = lax.broadcasted_iota(jnp.int32, (2 * rows, rows), 1)
                s = jnp.where(c <= r, s, -jnp.inf)
            new = jnp.broadcast_to(jnp.max(s, axis=-1, keepdims=True), (2 * rows, 128))
            if not first:
                old = top[i]
                new = jnp.maximum(old, new)
            terms = [jnp.exp2((s[:, c:c + 128] - new) * scale) for c in range(0, rows, 128)]
            weights = jnp.concatenate([e.astype(jnp.bfloat16) for e in terms], axis=1)
            pv = jnp.dot(weights, vals, preferred_element_type=jnp.float32)
            if first:
                acc[i] = pv
                total[i] = sum(terms)
            else:
                alpha = jnp.exp2((old - new) * scale)
                for c in range(0, VAL_DIM, 128):
                    acc[i, :, c:c + 128] = acc[i, :, c:c + 128] * alpha + pv[:, c:c + 128]
                total[i] = total[i] * alpha + sum(terms)
            top[i] = new

    fold(me, True)

    ways = ((0, above, below, me - 2), (1, below, above, me + 2))

    def tell_on(i, where):
        pl.semaphore_signal(chain.at[i], inc=1, device_id=(where, tp), device_id_type=MESH)

    if cap:
        for i, source, target, where in ways:
            @pl.when(jnp.logical_and(jnp.logical_not(source), target))
            def _():
                tell_on(i, where)

    if cap:
        choices, tokens = ids.shape
        which = lax.broadcasted_iota(jnp.int32, (max(n, 8), tokens), 0)
        named = [(ids[k:k + 1, :] == which).astype(jnp.float32) for k in range(choices)]
        before = lax.broadcasted_iota(jnp.int32, (tokens, tokens), 0) < lax.broadcasted_iota(
            jnp.int32, (tokens, tokens), 1
        )
        counts = jnp.dot(
            sum(named).astype(jnp.bfloat16), before.astype(jnp.bfloat16), preferred_element_type=jnp.float32
        )
        place = lax.broadcasted_iota(jnp.int32, (n * cap, tokens), 0)
        chosen = jnp.zeros((n * cap, tokens), jnp.float32)
        weight = jnp.zeros((n * cap, tokens), jnp.float32)
        for k in range(choices):
            rank = jnp.sum(named[k] * counts, axis=0, keepdims=True).astype(jnp.int32)
            hit = (ids[k:k + 1, :] * cap + rank) == place
            chosen = chosen + hit.astype(jnp.float32)
            weight = weight + jnp.where(hit, route[k:k + 1, :], 0.0)
        blend[...] = chosen.astype(jnp.bfloat16)
        weight = weight.T
        coarse = weight.astype(jnp.bfloat16)
        blend_back[:tokens] = coarse
        blend_back[tokens:] = (weight - coarse.astype(jnp.float32)).astype(jnp.bfloat16)

    def walk(d, _):
        z = zi - d
        @pl.when(d <= zi)
        def _():
            for c in range(HALVES):
                hop(z, c).wait_recv()
                y_copy(z, c).start()
                @pl.when(zi < nz - 1)
                def _():
                    hop(z, c).start()
            fold(2 * z + y, False)
        @pl.when(jnp.logical_or(d > 1, y == 1))
        def _():
            for c in range(HALVES):
                y_arrival(z + 1, c).wait_recv()
            fold(2 * (z + 1) + 1 - y, False)
        if cap:
            @pl.when((d == 1) & below & above)
            def _():
                for i, _, _, where in ways:
                    pl.semaphore_wait(chain.at[i], 1)
                    tell_on(i, where)
        return 0

    lax.fori_loop(1, jnp.where(zi + y > 0, zi + 2, 1), walk, 0)

    for h in range(2):
        r = pl.ds(h * rows, rows)
        one = acc[0, r, :] / jnp.sum(total[0, r, :], axis=-1, keepdims=True)
        two = acc[1, r, :] / jnp.sum(total[1, r, :], axis=-1, keepdims=True)
        diff = one - lam[:, h:h + 1] * two
        ms = jnp.mean(diff * diff, axis=-1, keepdims=True)
        heads[:, h * VAL_DIM:(h + 1) * VAL_DIM] = (
            diff * lax.rsqrt(ms + EPS) * gain[...] * OUT_SCALE
        ).astype(jnp.bfloat16)

    ow_load.wait()

    d_model = ow.shape[1]
    span = d_model // PARTS

    def picked(first, second):
        return jnp.concatenate(
            [heads[pl.ds(pl.multiple_of(t * chunk, chunk), chunk), :] for t in (first, second)], axis=0
        )

    def near_copy(q):
        cols = pl.ds(q * span, span)
        return remote(near_part.at[:, cols], near_got.at[:, cols], p_send.at[0], p_recv.at[0, q], near)

    def far_copy(q):
        cols = pl.ds(q * span, span)
        return remote(far_part.at[:, cols], far_got.at[:, cols], p_send.at[1], p_recv.at[1, q], far)

    away = 1 - side
    other = picked(2 * away + 1 - core, 2 * side + 1 - core)
    for q in range(PARTS):
        cols = slice(q * span, (q + 1) * span)
        near_part[:, cols] = jnp.dot(
            other, ow[:, cols], preferred_element_type=jnp.float32
        ).astype(jnp.bfloat16)
        near_copy(q).start()
    stream_load.wait()
    own = picked(2 * away + core, 2 * side + core)
    for q in range(PARTS):
        cols = slice(q * span, (q + 1) * span)
        mine = jnp.dot(own, ow[:, cols], preferred_element_type=jnp.float32)
        near_copy(q).wait_recv()
        mine = mine + near_got[:, cols].astype(jnp.float32)
        far_part[:, cols] = mine[:chunk].astype(jnp.bfloat16)
        far_copy(q).start()
        stream_out[:, cols] = stream[:, cols].astype(jnp.float32) + mine[chunk:]
    if cap:
        lax.fori_loop(ahead, 2 * DEEP, far_some, 0)
        for j in range(len(DOWN)):
            far_down(j).start()
    square = jnp.zeros((chunk, 1), jnp.float32)
    for q in range(PARTS):
        cols = slice(q * span, (q + 1) * span)
        far_copy(q).wait_recv()
        summed = stream_out[:, cols] + far_got[:, cols].astype(jnp.float32)
        stream_out[:, cols] = summed
        square = square + jnp.sum(summed * summed, axis=-1, keepdims=True)
    normed_out[...] = (
        stream_out[...] * lax.rsqrt(square * (1.0 / d_model) + EPS) * norm[...]
    ).astype(jnp.bfloat16)

    def finish_attention():
        remote(near_part, near_got, p_send.at[0], p_recv.at[0, 0], near).wait_send()
        remote(far_part, far_got, p_send.at[1], p_recv.at[1, 0], far).wait_send()

        for c in range(HALVES):
            @pl.when(y == 0)
            def _():
                y_copy(zi, c).wait_send()

            @pl.when(zi < nz - 1)
            def _():
                hop(zi, c).wait_send()

        def sent(z, _):
            for c in range(HALVES):
                y_copy(z, c).wait_send()
                @pl.when(zi < nz - 1)
                def _():
                    hop(z, c).wait_send()
            return 0

        lax.fori_loop(0, zi, sent, 0)

    if not cap:
        finish_attention()
        return

    def d_copy(s):
        return remote(send.at[s], rows_in.at[me], d_send.at[0], d_recv.at[zi], (s, tp))

    def d_arrival(first, count):
        some = pl.ds(first, count)
        return remote(send.at[some], rows_in.at[some], d_send.at[0], d_recv.at[first // 2], (pair, tp))

    others = pl.ds(0, n - 1)

    def r_copy(j, s):
        return remote(ret[j].at[s], back[j].at[me], r_send.at[0], r_recv.at[j], (s, tp))

    def r_arrival(j):
        return remote(ret[j].at[others], back[j].at[others], r_send.at[0], r_recv.at[j], (pair, tp))

    def dispatch(d, _):
        z = d
        base = pl.multiple_of(2 * z * cap, 2 * cap)
        got = jnp.dot(
            blend[pl.ds(base, 2 * cap), :], normed_out[...], preferred_element_type=jnp.float32
        ).astype(jnp.bfloat16)
        for j in range(2):
            s = 2 * z + j
            @pl.when(s != me)
            def _():
                send[s] = got[j * cap:(j + 1) * cap]
                d_copy(s).start()
            @pl.when(s == me)
            def _():
                rows_in[me] = got[j * cap:(j + 1) * cap]
        return 0

    for i, source, target, _ in ways:
        @pl.when(jnp.logical_and(source, jnp.logical_not(target)))
        def _():
            pl.semaphore_wait(chain.at[i], 1)
    lax.fori_loop(0, nz, dispatch, 0)

    def pass_on(p, _):
        far_piece(p).wait_recv()
        relay(p).start()
        return 0

    lax.fori_loop(0, DEEP, pass_on, 0)
    remote(third(0), third(ff), w_send.at[0], w_recv.at[0], near).wait_recv()
    local = 2 * ff

    def gated(x, cols):
        gate = jnp.dot(x, gu[0, :, cols], preferred_element_type=jnp.float32)
        upper = jnp.dot(x, gu[1, :, cols], preferred_element_type=jnp.float32)
        return (gate / (1.0 + jnp.exp(-gate)) * upper).astype(jnp.bfloat16)

    def work(z, _):
        lax.fori_loop(DEEP + z * (DEEP // nz), DEEP + (z + 1) * (DEEP // nz), pass_on, 0)
        @pl.when(z != zi)
        def _():
            d_arrival(2 * z, 2).wait_recv()
        @pl.when(z == zi)
        def _():
            d_arrival(pair, 1).wait_recv()
        x = rows_in[pl.ds(2 * z, 2)].reshape(2 * cap, d_model)
        base = pl.multiple_of(2 * z * cap, 2 * cap)
        hid[pl.ds(base, 2 * cap), :local] = gated(x, slice(0, local))
        return 0

    lax.fori_loop(0, nz, work, 0)

    def through(i):
        ends = gu.at[i, :, pl.ds(3 * ff, ff)]
        remote(ends, ends, g_send.at[0], g_recv.at[i], near).wait_recv()
        return jnp.dot(
            rows_in[...].reshape(n * cap, d_model), gu[i, :, local:], preferred_element_type=jnp.float32
        )

    gate = through(0)
    upper = through(1)
    hid[:, local:] = (gate / (1.0 + jnp.exp(-gate)) * upper).astype(jnp.bfloat16)

    def give_back(j):
        far_down(j).wait_recv()
        relay_down(j).start()
        relay_down(j).wait_recv()
        first, count = DOWN[j]
        down = jnp.dot(
            hid[...], dw[:, first * wide:(first + count) * wide], preferred_element_type=jnp.float32
        ).astype(jnp.bfloat16)
        ret[j][...] = down.reshape(n, cap, count * wide)
        back[j][me] = ret[j][me]

        def one(d, _):
            for k in range(2):
                s = 2 * jnp.where(zi >= nz // 2, d, nz - 1 - d) + k
                @pl.when(s != me)
                def _():
                    r_copy(j, s).start()
            return 0

        lax.fori_loop(0, nz, one, 0)

    def collect(j):
        r_arrival(j).wait_recv()
        first, count = DOWN[j]
        results = back[j][...].reshape(n * cap, count * wide)
        routed = jnp.dot(blend_back[...], results, preferred_element_type=jnp.float32)
        cols = slice(first * wide, (first + count) * wide)
        out_ref[:, cols] = (stream_out[:, cols] + routed[:tokens] + routed[tokens:]).astype(jnp.bfloat16)

    for j in range(len(DOWN)):
        give_back(j)
        if j > 1:
            collect(j - 2)
    finish_attention()
    remote(third(0), third(ff), w_send.at[0], w_recv.at[0], near).wait_send()
    remote(third(0), third(ff), f_send.at[0], f_recv.at[0], far).wait_send()
    remote(third(0), third(ff), g_send.at[0], g_recv.at[0], near).wait_send()
    remote(send.at[others], rows_in.at[others], d_send.at[0], d_recv.at[0], (pair, tp)).wait_send()
    remote(send.at[others], rows_in.at[others], r_send.at[0], r_recv.at[0], (pair, tp)).wait_send()

    for j in range(max(len(DOWN) - 2, 0), len(DOWN)):
        collect(j)


def layer(n, nt, cap, *args):
    q1, ow, stream_in = args[0], args[7], args[8]
    rows = q1.shape[0]
    tokens, d = stream_in.shape
    vm = pl.BlockSpec(memory_space=pltpu.VMEM)
    hbm = pl.BlockSpec(memory_space=pl.ANY)
    chunk = rows // nt
    dma = pltpu.SemaphoreType.DMA
    bf, f32 = jnp.bfloat16, jnp.float32
    in_specs = [hbm] * 10
    out_shape = (jax.ShapeDtypeStruct((tokens, d), f32), jax.ShapeDtypeStruct((tokens, d), bf))
    out_specs = (vm, vm)
    scratch = [
        pltpu.VMEM((n, rows, 2 * HEAD_DIM + VAL_DIM), bf),
        pltpu.VMEM((2, 2 * rows, HEAD_DIM), bf),
        pltpu.VMEM((2, 2 * rows, 128), f32),
        pltpu.VMEM((2, 2 * rows, 128), f32),
        pltpu.VMEM((2, 2 * rows, VAL_DIM), f32),
        pltpu.VMEM((rows, 2 * VAL_DIM), bf),
        pltpu.VMEM(ow.shape, bf),
        pltpu.VMEM((tokens, d), bf),
        pltpu.VMEM(args[5].shape, f32),
        pltpu.VMEM(args[6].shape, f32),
        pltpu.VMEM(args[9].shape, f32),
        pltpu.VMEM((2 * chunk, d), bf),
        pltpu.VMEM((2 * chunk, d), bf),
        pltpu.VMEM((chunk, d), bf),
        pltpu.VMEM((chunk, d), bf),
        dma((14,)), dma((n // 2 * HALVES,)), dma((n // 2 * HALVES,)), dma((n // 2 * HALVES,)), dma((n // 2 * HALVES,)), dma((2,)), dma((2, PARTS)),
    ]
    if cap:
        ff = args[12].shape[2]
        in_specs = in_specs + [hbm] * 5
        out_shape = pltpu.VMEM((tokens, d), bf)
        out_specs = vm
        scratch = scratch + [
            pltpu.VMEM((tokens, d), f32),
            pltpu.VMEM((tokens, d), bf),
            pltpu.VMEM((2, d, nt * ff), bf),
            pltpu.VMEM((nt * ff, d), bf),
            pltpu.VMEM((n * cap, tokens), bf),
            pltpu.VMEM((2 * tokens, n * cap), bf),
        ] + [pltpu.VMEM((n, cap, d), bf)] * 2 + [
            pltpu.VMEM((n * cap, nt * ff), bf),
            pltpu.VMEM(args[10].shape, jnp.int32),
            pltpu.VMEM(args[11].shape, f32),
            pltpu.SemaphoreType.REGULAR((2,)), dma((3,)), dma((1,)), dma((1,)),
        ] + [
            dma((1,)), dma((2 * DEEP + len(DOWN),)), dma((1,)), dma((2 + len(DOWN),)),
            dma((1,)), dma((n // 2,)), dma((1,)), dma((len(DOWN),)),
        ] + [pltpu.VMEM((n, cap, count * (d // WIDE)), bf) for _, count in DOWN] * 2
    return pl.pallas_call(
        functools.partial(layer_kernel, n, nt, cap),
        out_shape=out_shape,
        in_specs=in_specs,
        out_specs=out_specs,
        scratch_shapes=scratch,
        compiler_params=pltpu.CompilerParams(
            collective_id=0, has_side_effects=True, vmem_limit_bytes=58 * 2**20
        ),
        name="layer",
    )(*args)


def shards(
    stream_in,
    queries_one,
    queries_two,
    keys_one,
    keys_two,
    values,
    lambdas,
    head_gain,
    out_weight,
    norm_gain,
    expert_ids,
    route_weight,
    gate_weight,
    up_weight,
    down_weight,
):
    n, nt = lax.axis_size("sp"), lax.axis_size("tp")
    rows_here = stream_in.shape[0]
    top_count = expert_ids.shape[1]
    slot_cap = 2 * top_count * rows_here // n
    shared = (
        queries_one, queries_two, keys_one, keys_two, values, lambdas.reshape(1, -1),
        head_gain.reshape(1, -1), out_weight, stream_in, norm_gain.reshape(1, -1),
    )
    if slot_cap % 16 == 0:
        return layer(
            n, nt, slot_cap, *shared, expert_ids.T, route_weight.T, gate_weight, up_weight, down_weight
        )
    stream, normed = layer(n, nt, 0, *shared)
    flat_ids = expert_ids.reshape(-1)
    count = flat_ids.shape[0]
    order = lax.iota(jnp.int32, count)
    earlier = (flat_ids[None, :] == flat_ids[:, None]) & (order[None, :] < order[:, None])
    ranks = jnp.sum(earlier.astype(jnp.int32), axis=1)
    slots = flat_ids * slot_cap + ranks
    slot_of = slots.reshape(rows_here, top_count)
    places = lax.iota(jnp.int32, n * slot_cap)
    selector = sum(
        (slot_of[:, k][None, :] == places[:, None]).astype(jnp.bfloat16) for k in range(top_count)
    )
    send_rows = jnp.dot(selector, normed, preferred_element_type=jnp.float32).astype(jnp.bfloat16)
    received = lax.all_to_all(send_rows, "sp", split_axis=0, concat_axis=0, tiled=True)
    picked_rows = lax.all_gather(received, "tp", axis=0, tiled=True)
    gate = jnp.dot(picked_rows, gate_weight[0], preferred_element_type=jnp.float32)
    upper = jnp.dot(picked_rows, up_weight[0], preferred_element_type=jnp.float32)
    hidden = (jax.nn.silu(gate) * upper).astype(jnp.bfloat16)
    summed = lax.psum_scatter(
        jnp.dot(hidden, down_weight[0], preferred_element_type=jnp.float32).astype(jnp.bfloat16),
        "tp",
        scatter_dimension=0,
        tiled=True,
    )
    returned = lax.all_to_all(summed, "sp", split_axis=0, concat_axis=0, tiled=True)
    picked = jnp.take(returned, slots, axis=0).reshape(rows_here, top_count, -1).astype(jnp.float32)
    routed = jnp.sum(picked * route_weight[:, :, None], axis=1)
    return (stream + routed).astype(jnp.bfloat16)


def solution(mesh):
    return jax.shard_map(
        shards,
        mesh=mesh,
        in_specs=(
            P(("sp", "tp"), None),
            P("sp", "tp"),
            P("sp", "tp"),
            P("sp", "tp"),
            P("sp", "tp"),
            P("sp", "tp"),
            P("tp"),
            P(),
            P("tp", None),
            P(),
            P(("sp", "tp"), None),
            P(("sp", "tp"), None),
            P("sp", None, "tp"),
            P("sp", None, "tp"),
            P("sp", "tp", None),
        ),
        out_specs=P(("sp", "tp"), None),
        check_vma=False,
    )
```

```python
import functools

import jax
import jax.numpy as jnp
from jax import lax
from jax.experimental import pallas as pl
from jax.experimental.pallas import tpu as pltpu
from jax.sharding import PartitionSpec as P

HEAD_DIM = 128
VAL_DIM = 256


EPS = 1e-06
OUT_SCALE = 0.8


MESH = pl.DeviceIdType.MESH
LOG2E = 1.4426950408889634
DEEP = 8
WIDE = 16
DOWN = ((0, 2), (2, 2), (4, 2), (6, 2), (8, 2), (10, 2), (12, 2), (14, 2))
PARTS = 4
LAG = 3
HALVES = 2


def remote(src, dst, send_sem, recv_sem, where):
    return pltpu.make_async_remote_copy(
        src_ref=src,
        dst_ref=dst,
        send_sem=send_sem,
        recv_sem=recv_sem,
        device_id=where,
        device_id_type=MESH,
    )


def greet(devices, count):
    barrier = pltpu.get_barrier_semaphore()
    devices(lambda where: pl.semaphore_signal(barrier, inc=1, device_id=where, device_id_type=MESH))
    pl.semaphore_wait(barrier, count)


def layer_kernel(n, nt, cap, *refs):
    (
        q1_ref, q2_ref, k1_ref, k2_ref, v_ref, lam_ref, gain_ref, ow_ref, stream_ref, norm_ref,
    ) = refs[:10]
    if cap:
        ids_ref, route_ref, gw_ref, uw_ref, dw_ref, out_ref = refs[10:16]
        refs = refs[16:]
    else:
        stream_out, normed_out = refs[10:12]
        refs = refs[12:]
    kv, qs, top, total, acc, heads, ow, stream, lam, gain, norm, near_part, near_got, far_part, far_got = refs[:15]
    local_sem, z_send, z_recv, y_send, y_recv, p_send, p_recv = refs[15:22]
    if cap:
        (
            stream_out, normed_out, gu, dw, blend, blend_back, send, rows_in, hid,
            ids, route, chain, own_sem, w_send, w_recv, f_send, f_recv, g_send, g_recv, d_send, d_recv, r_send, r_recv,
        ) = refs[22:-2 * len(DOWN)]
        ret, back = refs[-2 * len(DOWN):-len(DOWN)], refs[-len(DOWN):]

    me, tp = lax.axis_index("sp"), lax.axis_index("tp")
    nz = n // 2
    zi, y = me // 2, lax.rem(me, 2)
    pair = me + 1 - 2 * y
    rows = q1_ref.shape[0]
    hd = HEAD_DIM
    chunk = rows // nt
    side, core = tp // 2, lax.rem(tp, 2)
    near = (me, tp + 1 - 2 * core)
    far = (me, lax.rem(tp + 2, 4))

    loads = [
        pltpu.make_async_copy(k1_ref, kv.at[me, :, pl.ds(0, hd)], local_sem.at[0]),
        pltpu.make_async_copy(k2_ref, kv.at[me, :, pl.ds(hd, hd)], local_sem.at[1]),
        pltpu.make_async_copy(v_ref, kv.at[me, :, pl.ds(2 * hd, VAL_DIM)], local_sem.at[2]),
    ]
    rest = [
        pltpu.make_async_copy(
            ref.at[:, pl.ds(h * hd, hd)], qs.at[i, pl.ds(h * rows, rows), :], local_sem.at[4 + 2 * i + h]
        )
        for i, ref in enumerate((q1_ref, q2_ref))
        for h in range(2)
    ]
    stream_load = pltpu.make_async_copy(stream_ref, stream, local_sem.at[8])
    small = [(lam_ref, lam), (gain_ref, gain), (norm_ref, norm)]
    if cap:
        small = small + [(ids_ref, ids), (route_ref, route)]
    small_loads = [
        pltpu.make_async_copy(ref, held, local_sem.at[9 + i]) for i, (ref, held) in enumerate(small)
    ]
    for load in loads + rest:
        load.start()
    stream_load.start()
    for load in small_loads:
        load.start()
    if cap:
        ff = gw_ref.shape[2]

        deep = gu.shape[1] // DEEP
        wide = dw.shape[1] // WIDE

        def part_of(i, k):
            if i == 2:
                return dw.at[pl.ds(k * ff, ff), :]
            return gu.at[i, :, pl.ds(k * ff, ff)]

        own_loads = [
            pltpu.make_async_copy(ref.at[0], part_of(i, 0), own_sem.at[i])
            for i, ref in enumerate((gw_ref, uw_ref, dw_ref))
        ]
        for load in own_loads:
            load.start()

        def w_copy(i):
            return remote(part_of(i, 0), part_of(i, 1), w_send.at[0], w_recv.at[0], near)

        def piece(p, k):
            rows_of = pl.ds(pl.multiple_of(lax.rem(p, DEEP) * deep, deep), deep)
            return gu.at[p // DEEP, rows_of, pl.ds(k * ff, ff)]

        def far_piece(p):
            return remote(piece(p, 0), piece(p, 2), f_send.at[0], f_recv.at[p], far)

        def relay(p):
            return remote(piece(p, 2), piece(p, 3), g_send.at[0], g_recv.at[p // DEEP], near)

        def down_piece(j, k):
            first, count = DOWN[j]
            return dw.at[pl.ds(k * ff, ff), pl.ds(first * wide, count * wide)]

        def far_down(j):
            p = 2 * DEEP + j
            return remote(down_piece(j, 0), down_piece(j, 2), f_send.at[0], f_recv.at[p], far)

        def relay_down(j):
            return remote(down_piece(j, 2), down_piece(j, 3), g_send.at[0], g_recv.at[2 + j], near)

        def third(k):
            return dw.at[pl.ds(k, 3 * ff), :]

        ahead = jnp.minimum(jnp.where(zi == 0, 5, jnp.where(zi == nz - 1, 10, 6 + zi)), 2 * DEEP)

        def far_some(p, _):
            far_piece(p).start()
            return 0

    ow_load = pltpu.make_async_copy(ow_ref, ow, local_sem.at[3])
    ow_load.start()

    below, above = zi > 0, zi < nz - 1

    def peers(tell):
        tell(near)
        tell(far)
        tell((pair, tp))
        @pl.when(below)
        def _():
            tell((me - 2, tp))
        @pl.when(above)
        def _():
            tell((me + 2, tp))

    greet(peers, 3 + below.astype(jnp.int32) + above.astype(jnp.int32))
    for load in loads:
        load.wait()

    part_rows = rows // HALVES

    def block(b, c):
        return kv.at[b, pl.ds(c * part_rows, part_rows), :]

    def hop(z, c):
        b, i = 2 * z + y, HALVES * z + c
        return remote(block(b, c), block(b, c), z_send.at[i], z_recv.at[i], (jnp.minimum(me + 2, n - 2 + y), tp))

    def y_copy(z, c):
        b, i = 2 * z + y, HALVES * z + c
        return remote(block(b, c), block(b, c), y_send.at[i], y_recv.at[i], (pair, tp))

    def y_arrival(z, c):
        b, i = 2 * z + 1 - y, HALVES * z + c
        return remote(block(b, c), block(b, c), y_send.at[i], y_recv.at[i], (pair, tp))

    for c in range(HALVES):
        @pl.when(zi < nz - 1)
        def _():
            hop(zi, c).start()

        @pl.when(y == 0)
        def _():
            y_copy(zi, c).start()

    if cap:
        own_loads[0].wait()
        own_loads[1].wait()
        lax.fori_loop(0, ahead, far_some, 0)
        own_loads[2].wait()
        for i in range(3):
            w_copy(i).start()

    for load in rest + small_loads:
        load.wait()

    scale = HEAD_DIM ** (-0.5) * LOG2E

    def fold(b, first):
        vals = kv[b, :, 2 * hd:]
        for i in range(2):
            keys = kv[b, :, i * hd:(i + 1) * hd]
            s = lax.dot_general(qs[i], keys, (((1,), (1,)), ((), ())), preferred_element_type=jnp.float32)
            if first:
                r = lax.broadcasted_iota(jnp.int32, (2, rows, rows), 1).reshape(2 * rows, rows)
                c = lax.broadcasted_iota(jnp.int32, (2 * rows, rows), 1)
                s = jnp.where(c <= r, s, -jnp.inf)
            new = jnp.broadcast_to(jnp.max(s, axis=-1, keepdims=True), (2 * rows, 128))
            if not first:
                old = top[i]
                new = jnp.maximum(old, new)
            terms = [jnp.exp2((s[:, c:c + 128] - new) * scale) for c in range(0, rows, 128)]
            weights = jnp.concatenate([e.astype(jnp.bfloat16) for e in terms], axis=1)
            pv = jnp.dot(weights, vals, preferred_element_type=jnp.float32)
            if first:
                acc[i] = pv
                total[i] = sum(terms)
            else:
                alpha = jnp.exp2((old - new) * scale)
                for c in range(0, VAL_DIM, 128):
                    acc[i, :, c:c + 128] = acc[i, :, c:c + 128] * alpha + pv[:, c:c + 128]
                total[i] = total[i] * alpha + sum(terms)
            top[i] = new

    fold(me, True)

    ways = ((0, above, below, me - 2), (1, below, above, me + 2))

    def tell_on(i, where):
        pl.semaphore_signal(chain.at[i], inc=1, device_id=(where, tp), device_id_type=MESH)

    if cap:
        for i, source, target, where in ways:
            @pl.when(jnp.logical_and(jnp.logical_not(source), target))
            def _():
                tell_on(i, where)

    if cap:
        choices, tokens = ids.shape
        which = lax.broadcasted_iota(jnp.int32, (max(n, 8), tokens), 0)
        named = [(ids[k:k + 1, :] == which).astype(jnp.float32) for k in range(choices)]
        before = lax.broadcasted_iota(jnp.int32, (tokens, tokens), 0) < lax.broadcasted_iota(
            jnp.int32, (tokens, tokens), 1
        )
        counts = jnp.dot(
            sum(named).astype(jnp.bfloat16), before.astype(jnp.bfloat16), preferred_element_type=jnp.float32
        )
        place = lax.broadcasted_iota(jnp.int32, (n * cap, tokens), 0)
        chosen = jnp.zeros((n * cap, tokens), jnp.float32)
        weight = jnp.zeros((n * cap, tokens), jnp.float32)
        for k in range(choices):
            rank = jnp.sum(named[k] * counts, axis=0, keepdims=True).astype(jnp.int32)
            hit = (ids[k:k + 1, :] * cap + rank) == place
            chosen = chosen + hit.astype(jnp.float32)
            weight = weight + jnp.where(hit, route[k:k + 1, :], 0.0)
        blend[...] = chosen.astype(jnp.bfloat16)
        weight = weight.T
        coarse = weight.astype(jnp.bfloat16)
        blend_back[:tokens] = coarse
        blend_back[tokens:] = (weight - coarse.astype(jnp.float32)).astype(jnp.bfloat16)

    def walk(d, _):
        z = zi - d
        @pl.when(d <= zi)
        def _():
            for c in range(HALVES):
                hop(z, c).wait_recv()
                y_copy(z, c).start()
                @pl.when(zi < nz - 1)
                def _():
                    hop(z, c).start()
            fold(2 * z + y, False)
        @pl.when(jnp.logical_or(d > 1, y == 1))
        def _():
            for c in range(HALVES):
                y_arrival(z + 1, c).wait_recv()
            fold(2 * (z + 1) + 1 - y, False)
        if cap:
            @pl.when((d == 1) & below & above)
            def _():
                for i, _, _, where in ways:
                    pl.semaphore_wait(chain.at[i], 1)
                    tell_on(i, where)
        return 0

    lax.fori_loop(1, jnp.where(zi + y > 0, zi + 2, 1), walk, 0)

    for h in range(2):
        r = pl.ds(h * rows, rows)
        one = acc[0, r, :] / jnp.sum(total[0, r, :], axis=-1, keepdims=True)
        two = acc[1, r, :] / jnp.sum(total[1, r, :], axis=-1, keepdims=True)
        diff = one - lam[:, h:h + 1] * two
        ms = jnp.mean(diff * diff, axis=-1, keepdims=True)
        heads[:, h * VAL_DIM:(h + 1) * VAL_DIM] = (
            diff * lax.rsqrt(ms + EPS) * gain[...] * OUT_SCALE
        ).astype(jnp.bfloat16)

    ow_load.wait()

    d_model = ow.shape[1]
    span = d_model // PARTS

    def picked(first, second):
        return jnp.concatenate(
            [heads[pl.ds(pl.multiple_of(t * chunk, chunk), chunk), :] for t in (first, second)], axis=0
        )

    def near_copy(q):
        cols = pl.ds(q * span, span)
        return remote(near_part.at[:, cols], near_got.at[:, cols], p_send.at[0], p_recv.at[0, q], near)

    def far_copy(q):
        cols = pl.ds(q * span, span)
        return remote(far_part.at[:, cols], far_got.at[:, cols], p_send.at[1], p_recv.at[1, q], far)

    away = 1 - side
    other = picked(2 * away + 1 - core, 2 * side + 1 - core)
    for q in range(PARTS):
        cols = slice(q * span, (q + 1) * span)
        near_part[:, cols] = jnp.dot(
            other, ow[:, cols], preferred_element_type=jnp.float32
        ).astype(jnp.bfloat16)
        near_copy(q).start()
    stream_load.wait()
    own = picked(2 * away + core, 2 * side + core)
    for q in range(PARTS):
        cols = slice(q * span, (q + 1) * span)
        mine = jnp.dot(own, ow[:, cols], preferred_element_type=jnp.float32)
        near_copy(q).wait_recv()
        mine = mine + near_got[:, cols].astype(jnp.float32)
        far_part[:, cols] = mine[:chunk].astype(jnp.bfloat16)
        far_copy(q).start()
        stream_out[:, cols] = stream[:, cols].astype(jnp.float32) + mine[chunk:]
    if cap:
        lax.fori_loop(ahead, 2 * DEEP, far_some, 0)
        for j in range(len(DOWN)):
            far_down(j).start()
    square = jnp.zeros((chunk, 1), jnp.float32)
    for q in range(PARTS):
        cols = slice(q * span, (q + 1) * span)
        far_copy(q).wait_recv()
        summed = stream_out[:, cols] + far_got[:, cols].astype(jnp.float32)
        stream_out[:, cols] = summed
        square = square + jnp.sum(summed * summed, axis=-1, keepdims=True)
    normed_out[...] = (
        stream_out[...] * lax.rsqrt(square * (1.0 / d_model) + EPS) * norm[...]
    ).astype(jnp.bfloat16)

    def finish_attention():
        remote(near_part, near_got, p_send.at[0], p_recv.at[0, 0], near).wait_send()
        remote(far_part, far_got, p_send.at[1], p_recv.at[1, 0], far).wait_send()

        for c in range(HALVES):
            @pl.when(y == 0)
            def _():
                y_copy(zi, c).wait_send()

            @pl.when(zi < nz - 1)
            def _():
                hop(zi, c).wait_send()

        def sent(z, _):
            for c in range(HALVES):
                y_copy(z, c).wait_send()
                @pl.when(zi < nz - 1)
                def _():
                    hop(z, c).wait_send()
            return 0

        lax.fori_loop(0, zi, sent, 0)

    if not cap:
        finish_attention()
        return

    def d_copy(s):
        return remote(send.at[s], rows_in.at[me], d_send.at[0], d_recv.at[zi], (s, tp))

    def d_arrival(first, count):
        some = pl.ds(first, count)
        return remote(send.at[some], rows_in.at[some], d_send.at[0], d_recv.at[first // 2], (pair, tp))

    others = pl.ds(0, n - 1)

    def r_copy(j, s):
        return remote(ret[j].at[s], back[j].at[me], r_send.at[0], r_recv.at[j], (s, tp))

    def r_arrival(j):
        return remote(ret[j].at[others], back[j].at[others], r_send.at[0], r_recv.at[j], (pair, tp))

    def dispatch(d, _):
        z = d
        base = pl.multiple_of(2 * z * cap, 2 * cap)
        got = jnp.dot(
            blend[pl.ds(base, 2 * cap), :], normed_out[...], preferred_element_type=jnp.float32
        ).astype(jnp.bfloat16)
        for j in range(2):
            s = 2 * z + j
            @pl.when(s != me)
            def _():
                send[s] = got[j * cap:(j + 1) * cap]
                d_copy(s).start()
            @pl.when(s == me)
            def _():
                rows_in[me] = got[j * cap:(j + 1) * cap]
        return 0

    for i, source, target, _ in ways:
        @pl.when(jnp.logical_and(source, jnp.logical_not(target)))
        def _():
            pl.semaphore_wait(chain.at[i], 1)
    lax.fori_loop(0, nz, dispatch, 0)

    def pass_on(p, _):
        far_piece(p).wait_recv()
        relay(p).start()
        return 0

    lax.fori_loop(0, DEEP, pass_on, 0)
    remote(third(0), third(ff), w_send.at[0], w_recv.at[0], near).wait_recv()
    local = 2 * ff

    def gated(x, cols):
        gate = jnp.dot(x, gu[0, :, cols], preferred_element_type=jnp.float32)
        upper = jnp.dot(x, gu[1, :, cols], preferred_element_type=jnp.float32)
        return (gate / (1.0 + jnp.exp(-gate)) * upper).astype(jnp.bfloat16)

    def work(z, _):
        lax.fori_loop(DEEP + z * (DEEP // nz), DEEP + (z + 1) * (DEEP // nz), pass_on, 0)
        @pl.when(z != zi)
        def _():
            d_arrival(2 * z, 2).wait_recv()
        @pl.when(z == zi)
        def _():
            d_arrival(pair, 1).wait_recv()
        x = rows_in[pl.ds(2 * z, 2)].reshape(2 * cap, d_model)
        base = pl.multiple_of(2 * z * cap, 2 * cap)
        hid[pl.ds(base, 2 * cap), :local] = gated(x, slice(0, local))
        return 0

    lax.fori_loop(0, nz, work, 0)

    def through(i):
        ends = gu.at[i, :, pl.ds(3 * ff, ff)]
        remote(ends, ends, g_send.at[0], g_recv.at[i], near).wait_recv()
        return jnp.dot(
            rows_in[...].reshape(n * cap, d_model), gu[i, :, local:], preferred_element_type=jnp.float32
        )

    gate = through(0)
    upper = through(1)
    hid[:, local:] = (gate / (1.0 + jnp.exp(-gate)) * upper).astype(jnp.bfloat16)

    def give_back(j):
        far_down(j).wait_recv()
        relay_down(j).start()
        relay_down(j).wait_recv()
        first, count = DOWN[j]
        down = jnp.dot(
            hid[...], dw[:, first * wide:(first + count) * wide], preferred_element_type=jnp.float32
        ).astype(jnp.bfloat16)
        ret[j][...] = down.reshape(n, cap, count * wide)
        back[j][me] = ret[j][me]

        def one(d, _):
            for k in range(2):
                s = 2 * jnp.where(zi >= nz // 2, d, nz - 1 - d) + k
                @pl.when(s != me)
                def _():
                    r_copy(j, s).start()
            return 0

        lax.fori_loop(0, nz, one, 0)

    def collect(j):
        r_arrival(j).wait_recv()
        first, count = DOWN[j]
        results = back[j][...].reshape(n * cap, count * wide)
        routed = jnp.dot(blend_back[...], results, preferred_element_type=jnp.float32)
        cols = slice(first * wide, (first + count) * wide)
        out_ref[:, cols] = (stream_out[:, cols] + routed[:tokens] + routed[tokens:]).astype(jnp.bfloat16)

    for j in range(len(DOWN)):
        give_back(j)
        if LAG <= j < len(DOWN) - 1:
            collect(j - LAG)
    finish_attention()
    remote(third(0), third(ff), w_send.at[0], w_recv.at[0], near).wait_send()
    remote(third(0), third(ff), f_send.at[0], f_recv.at[0], far).wait_send()
    remote(third(0), third(ff), g_send.at[0], g_recv.at[0], near).wait_send()
    remote(send.at[others], rows_in.at[others], d_send.at[0], d_recv.at[0], (pair, tp)).wait_send()
    remote(send.at[others], rows_in.at[others], r_send.at[0], r_recv.at[0], (pair, tp)).wait_send()

    for j in range(max(len(DOWN) - 1 - LAG, 0), len(DOWN)):
        collect(j)


def layer(n, nt, cap, *args):
    q1, ow, stream_in = args[0], args[7], args[8]
    rows = q1.shape[0]
    tokens, d = stream_in.shape
    vm = pl.BlockSpec(memory_space=pltpu.VMEM)
    hbm = pl.BlockSpec(memory_space=pl.ANY)
    chunk = rows // nt
    dma = pltpu.SemaphoreType.DMA
    bf, f32 = jnp.bfloat16, jnp.float32
    in_specs = [hbm] * 10
    out_shape = (jax.ShapeDtypeStruct((tokens, d), f32), jax.ShapeDtypeStruct((tokens, d), bf))
    out_specs = (vm, vm)
    scratch = [
        pltpu.VMEM((n, rows, 2 * HEAD_DIM + VAL_DIM), bf),
        pltpu.VMEM((2, 2 * rows, HEAD_DIM), bf),
        pltpu.VMEM((2, 2 * rows, 128), f32),
        pltpu.VMEM((2, 2 * rows, 128), f32),
        pltpu.VMEM((2, 2 * rows, VAL_DIM), f32),
        pltpu.VMEM((rows, 2 * VAL_DIM), bf),
        pltpu.VMEM(ow.shape, bf),
        pltpu.VMEM((tokens, d), bf),
        pltpu.VMEM(args[5].shape, f32),
        pltpu.VMEM(args[6].shape, f32),
        pltpu.VMEM(args[9].shape, f32),
        pltpu.VMEM((2 * chunk, d), bf),
        pltpu.VMEM((2 * chunk, d), bf),
        pltpu.VMEM((chunk, d), bf),
        pltpu.VMEM((chunk, d), bf),
        dma((14,)), dma((n // 2 * HALVES,)), dma((n // 2 * HALVES,)), dma((n // 2 * HALVES,)), dma((n // 2 * HALVES,)), dma((2,)), dma((2, PARTS)),
    ]
    if cap:
        ff = args[12].shape[2]
        in_specs = in_specs + [hbm] * 5
        out_shape = pltpu.VMEM((tokens, d), bf)
        out_specs = vm
        scratch = scratch + [
            pltpu.VMEM((tokens, d), f32),
            pltpu.VMEM((tokens, d), bf),
            pltpu.VMEM((2, d, nt * ff), bf),
            pltpu.VMEM((nt * ff, d), bf),
            pltpu.VMEM((n * cap, tokens), bf),
            pltpu.VMEM((2 * tokens, n * cap), bf),
        ] + [pltpu.VMEM((n, cap, d), bf)] * 2 + [
            pltpu.VMEM((n * cap, nt * ff), bf),
            pltpu.VMEM(args[10].shape, jnp.int32),
            pltpu.VMEM(args[11].shape, f32),
            pltpu.SemaphoreType.REGULAR((2,)), dma((3,)), dma((1,)), dma((1,)),
        ] + [
            dma((1,)), dma((2 * DEEP + len(DOWN),)), dma((1,)), dma((2 + len(DOWN),)),
            dma((1,)), dma((n // 2,)), dma((1,)), dma((len(DOWN),)),
        ] + [pltpu.VMEM((n, cap, count * (d // WIDE)), bf) for _, count in DOWN] * 2
    return pl.pallas_call(
        functools.partial(layer_kernel, n, nt, cap),
        out_shape=out_shape,
        in_specs=in_specs,
        out_specs=out_specs,
        scratch_shapes=scratch,
        compiler_params=pltpu.CompilerParams(
            collective_id=0, has_side_effects=True, vmem_limit_bytes=58 * 2**20
        ),
        name="layer",
    )(*args)


def shards(
    stream_in,
    queries_one,
    queries_two,
    keys_one,
    keys_two,
    values,
    lambdas,
    head_gain,
    out_weight,
    norm_gain,
    expert_ids,
    route_weight,
    gate_weight,
    up_weight,
    down_weight,
):
    n, nt = lax.axis_size("sp"), lax.axis_size("tp")
    rows_here = stream_in.shape[0]
    top_count = expert_ids.shape[1]
    slot_cap = 2 * top_count * rows_here // n
    shared = (
        queries_one, queries_two, keys_one, keys_two, values, lambdas.reshape(1, -1),
        head_gain.reshape(1, -1), out_weight, stream_in, norm_gain.reshape(1, -1),
    )
    if slot_cap % 16 == 0:
        return layer(
            n, nt, slot_cap, *shared, expert_ids.T, route_weight.T, gate_weight, up_weight, down_weight
        )
    stream, normed = layer(n, nt, 0, *shared)
    flat_ids = expert_ids.reshape(-1)
    count = flat_ids.shape[0]
    order = lax.iota(jnp.int32, count)
    earlier = (flat_ids[None, :] == flat_ids[:, None]) & (order[None, :] < order[:, None])
    ranks = jnp.sum(earlier.astype(jnp.int32), axis=1)
    slots = flat_ids * slot_cap + ranks
    slot_of = slots.reshape(rows_here, top_count)
    places = lax.iota(jnp.int32, n * slot_cap)
    selector = sum(
        (slot_of[:, k][None, :] == places[:, None]).astype(jnp.bfloat16) for k in range(top_count)
    )
    send_rows = jnp.dot(selector, normed, preferred_element_type=jnp.float32).astype(jnp.bfloat16)
    received = lax.all_to_all(send_rows, "sp", split_axis=0, concat_axis=0, tiled=True)
    picked_rows = lax.all_gather(received, "tp", axis=0, tiled=True)
    gate = jnp.dot(picked_rows, gate_weight[0], preferred_element_type=jnp.float32)
    upper = jnp.dot(picked_rows, up_weight[0], preferred_element_type=jnp.float32)
    hidden = (jax.nn.silu(gate) * upper).astype(jnp.bfloat16)
    summed = lax.psum_scatter(
        jnp.dot(hidden, down_weight[0], preferred_element_type=jnp.float32).astype(jnp.bfloat16),
        "tp",
        scatter_dimension=0,
        tiled=True,
    )
    returned = lax.all_to_all(summed, "sp", split_axis=0, concat_axis=0, tiled=True)
    picked = jnp.take(returned, slots, axis=0).reshape(rows_here, top_count, -1).astype(jnp.float32)
    routed = jnp.sum(picked * route_weight[:, :, None], axis=1)
    return (stream + routed).astype(jnp.bfloat16)


def solution(mesh):
    return jax.shard_map(
        shards,
        mesh=mesh,
        in_specs=(
            P(("sp", "tp"), None),
            P("sp", "tp"),
            P("sp", "tp"),
            P("sp", "tp"),
            P("sp", "tp"),
            P("sp", "tp"),
            P("tp"),
            P(),
            P("tp", None),
            P(),
            P(("sp", "tp"), None),
            P(("sp", "tp"), None),
            P("sp", None, "tp"),
            P("sp", None, "tp"),
            P("sp", "tp", None),
        ),
        out_specs=P(("sp", "tp"), None),
        check_vma=False,
    )
```
